512 devices in a mesh: ep: 32 (over z, x), tp: 16 (over y, core).
Axes of the slice: x: 4, y: 8, z: 8, core: 2. Of those that a mesh axis runs over, the one named last changes fastest.
Arguments:
- receptance: bfloat16 [16384, 1024], P('ep', 'tp'), may hold values from -6 to 6
- key_matrix: bfloat16 [16384, 1024], P('ep', 'tp'), may hold values from -6 to 6
- value_matrix: bfloat16 [16384, 1024], P('ep', 'tp'), may hold values from -6 to 6
- decay_data_term: bfloat16 [16384, 1024], P('ep', 'tp'), may hold values from -3.5 to 3.5
- correction_rate_data: bfloat16 [16384, 1024], P('ep', 'tp'), may hold values from -6 to 6
- output_gate_input: bfloat16 [16384, 1024], P('ep', 'tp'), may hold values from -6 to 6
- decay_channel_offset: float32 [1024], P('tp'), may hold values from -12 to -2
- correction_rate_offset: float32 [1024], P('tp'), may hold values from -12 to 1
- extra_head_log_decay: float32 [16384, 16], P('ep', 'tp'), may hold values from -2.1 to 0, as said below
- head_norm_gain: float32 [1024], P('tp'), may hold values from 0.1 to 1.9
- mixer_output_weight: bfloat16 [1024, 2048], P('tp'), may hold values from -0.1875 to 0.1875
- expert_layer_input: bfloat16 [4096, 2048], P('ep'), may hold values from -6 to 6
- feedforward_norm_gain: float32 [2048], replicated, may hold values from 0.1 to 1.9
- group_router_weight: bfloat16 [2048, 4], replicated, may hold values from -0.125 to 0.125
- expert_router_weight: bfloat16 [2048, 32], replicated, may hold values from -0.125 to 0.125
- routes: int32 [4096, 2], P('ep'), may hold values from 0 to 31, all different within a row; in each aligned block of 128 rows (0 to 127, 128 to 255, ...) at most 16 rows name the same one
- expert_gate_weight: bfloat16 [32, 2048, 4096], P('ep', None, 'tp'), may hold values from -0.125 to 0.125
- expert_up_weight: bfloat16 [32, 2048, 4096], P('ep', None, 'tp'), may hold values from -0.125 to 0.125
- expert_down_weight: bfloat16 [32, 4096, 2048], P('ep', 'tp'), may hold values from -0.09375 to 0.09375
Outputs:
- token_mixer_output: bfloat16 [16384, 2048], P(('ep', 'tp'))
- expert_out: bfloat16 [4096, 2048], P('ep', 'tp')
The draws below stay inside these ranges and needn't reach their ends.
Inputs may be any that keep to these rules, and one draw needn't show every extreme that they name: A token's routes are distinct. Within the rows of one index of ep, no expert is named by more than 16 rows, a bound that some block reaches. `extra_head_log_decay`: entries are zero or negative; each head has a few nonzero positions.
All inputs are finite; a program needn't handle non-finite values.
Results may differ from the reference program's by a relative error of at most 0.022.
Values may be sent and summed in bfloat16 or wider, within the bound.
A program may use at most 64 MiB of HBM per device.

```python
import math
import jax
import jax.numpy as jnp
import numpy as np
from jax import lax

D = 2048
HEAD_DIM = 64
HEADS = 16
MIX = 1024
FF = 4096
GROUPS = 4
EXPERTS = 32
TOP = 2
MIX_ROWS = 512
MIX_TOKENS = 16384
MOE_ROWS = 128
MOE_TOKENS = 4096
CAP = 16
N_EP = 32
N_TP = 16


def slow_heads(key):
    share = 0.5
    return jax.random.uniform(jax.random.fold_in(key, 101), (HEADS,)) < share


def draw_decay_channel_offset(key, part):
    slow = slow_heads(key)
    slow_level = math.log(0.5 / MIX_TOKENS) + 0.5
    fast_level = math.log(0.03) + 0.5
    level = jnp.where(slow, slow_level, fast_level)
    jitter = jax.random.uniform(jax.random.fold_in(key, 3), (HEADS, HEAD_DIM), jnp.float32, -0.3, 0.3)
    return (level[:, None] + jitter).reshape(MIX).astype(jnp.float32)


def draw_correction_rate_offset(key, part):
    slow = slow_heads(key)
    slow_level = math.log(6.0 / MIX_TOKENS)
    spread = jax.random.uniform(jax.random.fold_in(key, 5), (HEADS, HEAD_DIM), jnp.float32, -1.0, 1.0)
    level = jnp.where(slow[:, None], slow_level + 0.3 * spread, spread)
    return level.reshape(MIX).astype(jnp.float32)


def draw_decay_data_term(key, part):
    blocks = MIX_TOKENS // MIX_ROWS
    offset = jax.random.uniform(jax.random.fold_in(key, 7), (blocks, 1, HEADS, 1), jnp.float32, -0.4, 0.4)
    noise = 0.5 * jax.random.normal(jax.random.fold_in(key, 9), (blocks, MIX_ROWS, HEADS, HEAD_DIM), jnp.float32)
    return (offset + noise).reshape(MIX_TOKENS, MIX).astype(jnp.bfloat16)


def draw_extra_head_log_decay(key, part):
    where_at = jax.random.randint(jax.random.fold_in(key, 13), (3, HEADS), 0, MIX_TOKENS)
    depth = jnp.log(jax.random.uniform(jax.random.fold_in(key, 17), (3, HEADS), jnp.float32, 0.5, 0.8))
    positions = jnp.arange(MIX_TOKENS)[:, None, None]
    struck = positions == where_at[None, :, :]
    return jnp.sum(jnp.where(struck, depth[None, :, :], 0.0), axis=1).astype(jnp.float32)


def levels(rng, extent, shards, low, high):
    loudness, own = 1.0, jax.random.fold_in(rng, 6)
    for position, blocks in shards:
        draws = jnp.exp(jax.random.uniform(jax.random.fold_in(own, position), (blocks,), jnp.float32, low / len(shards), high / len(shards)))
        loudness = loudness * jnp.repeat(draws, extent[position] // blocks).reshape([-1 if axis == position else 1 for axis in range(len(extent))])
    return loudness


def routed_block(own_key, own, number, rows, count, top, reach, skew):
    sequence = jax.random.permutation(own_key, count)
    heavy_load, ordinary = shares(count, rows * top, reach, skew, True), shares(count, rows * top, reach, skew, False)
    places = jnp.arange(count)

    def named(tallies, offset_by):
        used = int((tallies > 0).sum())
        fixed = max(1, used // 4)
        shifted = fixed + (places - fixed + offset_by * (used - fixed)) % max(1, count - fixed)
        return jnp.zeros((count,), jnp.int32).at[sequence[jnp.where(places < fixed, places, shifted)]].set(jnp.asarray(tallies, jnp.int32))

    tallies = jnp.where(number % 4 == 0, named(heavy_load, number // 4), named(ordinary, number - number // 4 - 1))
    mixed = jax.random.permutation(jax.random.fold_in(own, 3), count)
    giver, sink = mixed[0:count // 2 * 2:2], mixed[1:count // 2 * 2:2]
    margin = jnp.minimum(tallies[giver] - 1, reach - tallies[sink]) // 2
    margin = jnp.where((giver == sequence[0]) | (sink == sequence[0]) | (tallies[sink] == 0), 0, jnp.maximum(margin, 0))
    shifted = jax.random.randint(jax.random.fold_in(own, 4), (count // 2,), 0, 1 << 20) % (margin + 1)
    tallies = tallies.at[giver].add(-shifted).at[sink].add(shifted)
    labels = jnp.searchsorted(jnp.cumsum(tallies), jnp.arange(rows * top), side="right").astype(jnp.int32)
    table = labels.reshape(top, rows).T
    table = table[jax.random.permutation(jax.random.fold_in(own, 1), rows)]
    offset_by = jax.random.randint(jax.random.fold_in(own, 2), (rows, 1), 0, top)
    return jnp.take_along_axis(table, (jnp.arange(top)[None, :] + offset_by) % top, axis=1)


def shares(amount, total, bound, lean, full):
    portions = [(1 << 20) // math.isqrt(standing ** lean) + 1 for standing in range(1, amount + 1)]
    largest = bound if full else min(bound, max(-(-total // amount), total * portions[0] // sum(portions)))
    least = 1 if total - largest >= amount - 1 else 0
    counts, surplus = [largest] + [least] * (amount - 1), total - largest - least * (amount - 1)
    while surplus > 0:
        movable = [i for i in range(1, amount) if counts[i] < largest] or [i for i in range(1, amount) if counts[i] < bound]
        pool, remaining = sum([portions[i] for i in movable]), surplus
        for i in movable:
            addition = min(bound - counts[i], max(1, remaining * portions[i] // pool), surplus)
            counts[i] = counts[i] + addition
            surplus = surplus - addition
    return np.array(counts)


def centred(key, shape, scale, reach, pieces=(), held_as=jnp.bfloat16):
    drawn = scale * jax.random.normal(key, shape, jnp.float32)
    if pieces:
        drawn = drawn * levels(key, shape, pieces, -0.22, 0.18)
    return jnp.clip(drawn, -reach, reach).astype(held_as)


def setup_inputs(seed: int = 0) -> dict:
    splits = jax.random.split(jax.random.key(seed), 20)
    receptance = centred(splits[0], (MIX_TOKENS, MIX), 1.0, 6.0, ((0, 32), (1, 16)))
    key_matrix = centred(splits[1], (MIX_TOKENS, MIX), 1.0, 6.0, ((0, 32), (1, 16)))
    value_matrix = centred(splits[2], (MIX_TOKENS, MIX), 1.0, 6.0, ((0, 32), (1, 16)))
    decay_data_term = draw_decay_data_term(jax.random.fold_in(splits[19], 71), 0)
    correction_rate_data = centred(splits[4], (MIX_TOKENS, MIX), 1.0, 6.0, ((0, 32), (1, 16)))
    output_gate_input = centred(splits[5], (MIX_TOKENS, MIX), 1.0, 6.0, ((0, 32), (1, 16)))
    decay_channel_offset = draw_decay_channel_offset(jax.random.fold_in(splits[19], 71), 0)
    correction_rate_offset = draw_correction_rate_offset(jax.random.fold_in(splits[19], 71), 0)
    extra_head_log_decay = draw_extra_head_log_decay(jax.random.fold_in(splits[19], 71), 0)
    head_norm_gain = jnp.clip(1.0 + 0.18 * jax.random.normal(splits[9], (MIX,), jnp.float32), 0.1, 1.9)
    mixer_output_weight = centred(splits[10], (MIX, D), MIX ** -0.5, 0.1875, ((0, 16),))
    expert_layer_input = centred(splits[11], (MOE_TOKENS, D), 1.0, 6.0, ((0, 32),))
    feedforward_norm_gain = jnp.clip(1.0 + 0.18 * jax.random.normal(splits[12], (D,), jnp.float32), 0.1, 1.9)
    group_router_weight = centred(splits[13], (D, GROUPS), D ** -0.5, 0.125)
    expert_router_weight = centred(splits[14], (D, EXPERTS), D ** -0.5, 0.125)
    routes_keys = jax.random.split(jax.random.fold_in(splits[15], 1), MOE_TOKENS // MOE_ROWS)
    routes_turns = jax.random.permutation(jax.random.fold_in(splits[15], 3), MOE_TOKENS // MOE_ROWS)
    routes = jax.vmap(lambda own, number: routed_block(jax.random.fold_in(splits[15], 2), own, number, MOE_ROWS, EXPERTS, TOP, CAP, 2))(routes_keys, routes_turns).reshape((MOE_TOKENS, TOP))
    expert_gate_weight = centred(splits[16], (EXPERTS, D, FF), D ** -0.5, 0.125, ((0, 32), (2, 16)))
    expert_up_weight = centred(splits[17], (EXPERTS, D, FF), D ** -0.5, 0.125, ((0, 32), (2, 16)))
    expert_down_weight = centred(splits[18], (EXPERTS, FF, D), FF ** -0.5, 0.09375, ((0, 32), (1, 16)))
    return {"receptance": receptance, "key_matrix": key_matrix, "value_matrix": value_matrix, "decay_data_term": decay_data_term, "correction_rate_data": correction_rate_data, "output_gate_input": output_gate_input, "decay_channel_offset": decay_channel_offset, "correction_rate_offset": correction_rate_offset, "extra_head_log_decay": extra_head_log_decay, "head_norm_gain": head_norm_gain, "mixer_output_weight": mixer_output_weight, "expert_layer_input": expert_layer_input, "feedforward_norm_gain": feedforward_norm_gain, "group_router_weight": group_router_weight, "expert_router_weight": expert_router_weight, "routes": routes, "expert_gate_weight": expert_gate_weight, "expert_up_weight": expert_up_weight, "expert_down_weight": expert_down_weight}


key_eps = 1e-06
group_eps = 0.00064
norm_eps = 1e-06
highest = lax.Precision.HIGHEST

def token_mixer_block(receptance, key_matrix, value_matrix, decay_data_term, correction_rate_data, output_gate_input, decay_channel_offset, correction_rate_offset, extra_head_log_decay, head_norm_gain, mixer_output_weight):
    positions = receptance.shape[0]

    def head_view(tensor_in):
        return tensor_in.astype(jnp.float32).reshape(positions, HEADS, HEAD_DIM)
    recept = head_view(receptance)
    keyed = head_view(key_matrix)
    valued = head_view(value_matrix)
    unit_keys = keyed * lax.rsqrt(lax.optimization_barrier(jnp.sum(keyed * keyed, axis=-1, keepdims=True)) + key_eps)
    learn_rate = jax.nn.sigmoid(head_view(correction_rate_data) + correction_rate_offset.reshape(HEADS, HEAD_DIM))
    decay_preactivation = head_view(decay_data_term) + decay_channel_offset.reshape(HEADS, HEAD_DIM)
    decay_factor = jnp.exp(-jnp.exp(-jax.nn.softplus(-decay_preactivation) - 0.5) + extra_head_log_decay[:, :, None])
    removal = unit_keys * learn_rate

    def advance(state, inputs):
        recept_now, decay_now, unit_now, removal_now, key_now, value_now = inputs
        along = jnp.einsum('hvk,hk->hv', state, unit_now, precision=highest)
        state = state * decay_now[:, None, :] - along[:, :, None] * removal_now[:, None, :] + value_now[:, :, None] * key_now[:, None, :]
        return (state, jnp.einsum('hvk,hk->hv', state, recept_now, precision=highest))
    start_state = jnp.zeros((HEADS, HEAD_DIM, HEAD_DIM), jnp.float32)
    _, head_out = lax.scan(advance, start_state, (recept, decay_factor, unit_keys, removal, keyed, valued))
    centre = lax.optimization_barrier(jnp.mean(head_out, axis=-1, keepdims=True))
    spread = lax.optimization_barrier(jnp.mean(jnp.square(head_out - centre), axis=-1, keepdims=True))
    normed = (head_out - centre) * lax.rsqrt(spread + group_eps)
    gated = normed * head_norm_gain.reshape(HEADS, HEAD_DIM) * jax.nn.sigmoid(head_view(output_gate_input))
    mixed_hidden = gated.reshape(positions, MIX).astype(jnp.bfloat16)
    hidden_groups = jnp.moveaxis(mixed_hidden.reshape(positions, N_TP, MIX // N_TP), 1, 0)
    weight_groups = mixer_output_weight.reshape(N_TP, MIX // N_TP, D)

    def add_group(total, pair):
        block_hidden, block_weight = pair
        part = jnp.dot(block_hidden, block_weight, preferred_element_type=jnp.float32).astype(jnp.bfloat16)
        part = lax.optimization_barrier(part)
        return (total + part.astype(jnp.float32), None)
    total, _ = lax.scan(add_group, jnp.zeros((positions, D), jnp.float32), (hidden_groups, weight_groups))
    return total.astype(jnp.bfloat16)

def expert_block(expert_layer_input, feedforward_norm_gain, group_router_weight, expert_router_weight, routes, expert_gate_weight, expert_up_weight, expert_down_weight):
    tokens = expert_layer_input.shape[0]
    widened = expert_layer_input.astype(jnp.float32)
    normed_input = (widened * lax.rsqrt(lax.optimization_barrier(jnp.mean(widened * widened, axis=-1, keepdims=True)) + norm_eps) * feedforward_norm_gain).astype(jnp.bfloat16)
    group_logit = jnp.dot(normed_input, group_router_weight, preferred_element_type=jnp.float32)
    group_exp = jnp.exp(group_logit)
    group_prob = group_exp / lax.optimization_barrier(jnp.sum(group_exp, axis=-1, keepdims=True))
    expert_logit = jnp.dot(normed_input, expert_router_weight, preferred_element_type=jnp.float32)
    per_group = EXPERTS // GROUPS
    chosen_logit = jnp.take_along_axis(expert_logit, routes, axis=1)
    chosen_group = jnp.take_along_axis(group_prob, routes // per_group, axis=1)
    route_weight = chosen_group * jax.nn.sigmoid(chosen_logit - chosen_logit[:, ::-1])
    flat_routes = routes.reshape(-1)
    onehot = (flat_routes[:, None] == jnp.arange(EXPERTS, dtype=jnp.int32)[None, :]).astype(jnp.int32)
    ranked = lax.optimization_barrier(jnp.sum((jnp.cumsum(onehot, axis=0) - onehot) * onehot, axis=1))
    room = N_EP * CAP
    destination = (flat_routes * room + ranked).astype(jnp.int32)
    source_rows = jnp.zeros((EXPERTS * room,), jnp.int32).at[destination].set((jnp.arange(flat_routes.shape[0], dtype=jnp.int32) // TOP).astype(jnp.int32))
    gathered = normed_input[source_rows].reshape(EXPERTS, room, D)

    def run_expert(pack):
        rows_in, gate_mat, up_mat, down_mat = pack
        gate_val = jnp.dot(rows_in, gate_mat, preferred_element_type=jnp.float32)
        up_val = jnp.dot(rows_in, up_mat, preferred_element_type=jnp.float32)
        expert_hidden = (jax.nn.silu(gate_val) * up_val).astype(jnp.bfloat16)
        hidden_groups = expert_hidden.reshape(room, N_TP, FF // N_TP)
        down_groups = down_mat.reshape(N_TP, FF // N_TP, D)
        total = jnp.zeros((room, D), jnp.float32)
        for member in range(N_TP):
            part = jnp.dot(hidden_groups[:, member], down_groups[member], preferred_element_type=jnp.float32).astype(jnp.bfloat16)
            part = lax.optimization_barrier(part)
            total = total + part.astype(jnp.float32)
        return total.astype(jnp.bfloat16)
    expert_rows = lax.map(run_expert, (gathered, expert_gate_weight, expert_up_weight, expert_down_weight)).reshape(EXPERTS * room, D)
    picked = expert_rows[destination].astype(jnp.float32).reshape(tokens, TOP, D)
    return lax.optimization_barrier(jnp.sum(picked * route_weight[:, :, None], axis=1)).astype(jnp.bfloat16)

def reference(receptance, key_matrix, value_matrix, decay_data_term, correction_rate_data, output_gate_input, decay_channel_offset, correction_rate_offset, extra_head_log_decay, head_norm_gain, mixer_output_weight, expert_layer_input, feedforward_norm_gain, group_router_weight, expert_router_weight, routes, expert_gate_weight, expert_up_weight, expert_down_weight):
    token_mixer_output = token_mixer_block(receptance, key_matrix, value_matrix, decay_data_term, correction_rate_data, output_gate_input, decay_channel_offset, correction_rate_offset, extra_head_log_decay, head_norm_gain, mixer_output_weight)
    expert_out = expert_block(expert_layer_input, feedforward_norm_gain, group_router_weight, expert_router_weight, routes, expert_gate_weight, expert_up_weight, expert_down_weight)
    return (token_mixer_output, expert_out)
```

```python
import functools
import jax
import jax.numpy as jnp
from jax import lax
from jax.experimental import pallas as pl
from jax.experimental.pallas import tpu as pltpu
from jax.sharding import PartitionSpec as P

HEAD_DIM = 64
GROUPS = 4


key_eps = 1e-06
group_eps = 0.00064
norm_eps = 1e-06


def sent_to_all(value, axis):
    devices = lax.axis_size(axis)
    return lax.all_to_all(
        jnp.broadcast_to(value[None], (devices, *value.shape)), axis, 0, 0, tiled=True
    )


def all_in_one(value, axis):
    leaves = jax.tree.leaves(value)
    sequence = sorted(range(len(leaves)), key=lambda k: -leaves[k].size)
    width = (1, *leaves[sequence[0]].shape)[-1]
    lines = [
        jnp.pad(leaves[k].reshape(-1), (0, -leaves[k].size % width)).reshape(-1, width)
        for k in sequence
    ]
    both, at, found = (sent_to_all(jnp.concatenate(lines), axis), 0, {})
    for k, line in zip(sequence, lines):
        piece = both[:, at : at + len(line)].reshape(len(both), -1)
        found[k] = piece[:, : leaves[k].size].reshape(-1, *leaves[k].shape)
        at += len(line)
    numbers = iter(range(len(leaves)))
    return jax.tree.map(lambda _: found[next(numbers)], value)


def folded_in_pairs(pieces, combine):
    while len(jax.tree.leaves(pieces)[0]) > 1:
        pieces = jax.vmap(combine)(
            *(jax.tree.map(lambda part: part[side::2], pieces) for side in (0, 1))
        )
    return jax.tree.map(lambda part: part[0], pieces)


def entering(value, axis, combine, identity):
    devices, place = (lax.axis_size(axis), lax.axis_index(axis))
    passed = jnp.arange(devices) < place

    def kept(part, zero, own):
        part = jnp.where(
            passed.reshape(-1, *(1 for _ in own.shape)),
            part.astype(own.dtype),
            jnp.asarray(zero, own.dtype),
        )
        return part

    pieces = all_in_one(
        jax.tree.map(lambda part, kind: part.astype(kind), value, (jnp.bfloat16, jnp.bfloat16)),
        axis,
    )
    return folded_in_pairs(jax.tree.map(kept, pieces, identity, value), combine)


def in_blocks(value, dim, devices):
    before, after = (value.shape[:dim], value.shape[dim + 1 :])
    return jnp.moveaxis(value.reshape(*before, devices, -1, *after), dim, 0)


def summed_on_arrival(value, axis, dim):
    parts = in_blocks(value, dim, lax.axis_size(axis))
    arrived = lax.all_to_all(parts, axis, split_axis=0, concat_axis=0, tiled=True)
    return arrived.astype(jnp.float32).sum(axis=0)


HD=64
f32=jnp.float32; bf16=jnp.bfloat16
NN=(((1,),(0,)),((),())); NT=(((1,),(1,)),((),())); TN=(((0,),(0,)),((),()))
def dotb(a,b,dims=NN):
    return lax.dot_general(a.astype(bf16), b.astype(bf16), dims, preferred_element_type=f32)
def dot3(a,b,dims=NN):
    ah=a.astype(bf16); bh=b.astype(bf16)
    al=(a-ah.astype(f32)).astype(bf16); bl=(b-bh.astype(f32)).astype(bf16)
    d=lambda p,q: lax.dot_general(p,q,dims,preferred_element_type=f32)
    return d(ah,bh)+(d(ah,bl)+d(al,bh))
def dot2(a,b,dims=NN):
    ah=a.astype(bf16); bh=b.astype(bf16); bl=(b-bh.astype(f32)).astype(bf16)
    d=lambda p,q: lax.dot_general(p,q,dims,preferred_element_type=f32)
    return d(ah,bh)+d(ah,bl)
def sigmoid(x): return 1.0/(1.0+jnp.exp(-x))
def chunk_local(r,k,v,dd,cr,doff,coff,extra, inv_dot=dot3):
    C=r.shape[0]
    row=lax.broadcasted_iota(jnp.int32,(C,C),0); col=lax.broadcasted_iota(jnp.int32,(C,C),1)
    u=k*lax.rsqrt(jnp.sum(k*k,axis=-1,keepdims=True)+1e-6)
    a=u*sigmoid(cr+coff)
    lg=extra-0.6065306597126334*sigmoid(dd+doff)
    tri=jnp.where(row>=col,1.0,0.0)
    lh=lg.astype(bf16); l2=lg-lh.astype(f32); lm=l2.astype(bf16); ll=(l2-lm.astype(f32)).astype(bf16)
    tb=tri.astype(bf16)
    d=lambda q: lax.dot_general(tb,q,NN,preferred_element_type=f32)
    cum=d(lh)+(d(lm)+d(ll))
    bef=cum-lg
    tot=cum[C-1:C,:]
    ref=0.5*tot
    en=jnp.exp(ref-cum)
    lhs=jnp.concatenate([u*jnp.exp(bef-ref), r*jnp.exp(cum-ref)],axis=0)
    rhs=jnp.concatenate([k*en, a*en],axis=0)
    G=dotb(lhs,rhs,NT)
    strict=row>col; upto=row>=col
    kp=jnp.where(strict,G[:C,:C],0.0); A=jnp.where(strict,G[:C,C:],0.0)
    rk=jnp.where(upto,G[C:,:C],0.0); rr=jnp.where(upto,G[C:,C:],0.0)
    x=row^col
    T=jnp.where(row==col,1.0,0.0)-jnp.where(x==1,A,0.0)
    s=2
    while s<C:
        m=jnp.where((x>=s)&(x<2*s),A,0.0)
        T=T-inv_dot(T,inv_dot(m,T))
        s*=2
    kv=dotb(jnp.concatenate([kp,rk],axis=0),v)
    R=jnp.concatenate([kv[:C],u*jnp.exp(bef)],axis=1)
    X=dotb(T,R)
    out=jnp.concatenate([kv[C:],r*jnp.exp(cum)],axis=1)-dotb(rr,X)
    tail=jnp.exp(tot-cum)
    r64=lax.broadcasted_iota(jnp.int32,(HD,HD),0); c64=lax.broadcasted_iota(jnp.int32,(HD,HD),1)
    diag=jnp.where(r64==c64,jnp.exp(tot),0.0)
    BM=jnp.concatenate([dotb(k*tail,v,TN),diag],axis=1)-dotb(a*tail,X,TN)
    return out,BM

def chain_join(earlier, later):
    joined_map = jnp.einsum("vk,kj->vj", later[0], earlier[0])
    joined_state = jnp.einsum("vk,kj->vj", later[0], earlier[1]) + later[1]
    return (joined_map, joined_state)


def local_kernel(r, k, v, dd, cr, doff, coff, extra, out_ref, qp_ref, dev_ref):
    C = 128
    parts = []
    for c in range(4):
        s = slice(c * C, (c + 1) * C)
        out, bm = chunk_local(
            r[s].astype(f32), k[s].astype(f32), v[s].astype(f32), dd[s].astype(f32),
            cr[s].astype(f32), doff[...], coff[...], extra[s],
        )
        out_ref[s] = out
        parts.append(bm)
    r64 = lax.broadcasted_iota(jnp.int32, (HD, 2 * HD), 0)
    c64 = lax.broadcasted_iota(jnp.int32, (HD, 2 * HD), 1)
    qp = jnp.where(c64 == r64 + HD, 1.0, 0.0)
    for c in range(4):
        qp_ref[c] = qp
        bm = parts[c]
        qp = dot3(bm[:, HD:], qp) + jnp.where(c64 < HD, bm, 0.0)
    dev_ref[...] = qp.astype(bf16)


def finish_kernel(out_ref, qp_ref, z_ref, gate, gain, mixed_ref):
    C = 128
    z = z_ref[...]
    for c in range(4):
        s = slice(c * C, (c + 1) * C)
        qp = qp_ref[c]
        zc = dot2(qp[:, HD:], z) + qp[:, :HD]
        out = out_ref[s]
        ho = out[:, :HD] + dotb(out[:, HD:], zc)
        ho = ho - jnp.mean(ho, axis=-1, keepdims=True)
        sp = jnp.mean(ho * ho, axis=-1, keepdims=True)
        g = sigmoid(gate[s].astype(f32))
        mixed_ref[s] = (ho * lax.rsqrt(sp + group_eps) * gain[...] * g).astype(bf16)


def mixer_part(
    receptance,
    key_matrix,
    value_matrix,
    decay_data_term,
    correction_rate_data,
    output_gate_input,
    decay_channel_offset,
    correction_rate_offset,
    extra_head_log_decay,
    head_norm_gain,
    mixer_output_weight,
):
    rows = receptance.shape[0]
    out, qp, dev = pl.pallas_call(
        local_kernel,
        out_shape=(
            jax.ShapeDtypeStruct((rows, 2 * HD), f32),
            jax.ShapeDtypeStruct((4, HD, 2 * HD), f32),
            jax.ShapeDtypeStruct((HD, 2 * HD), bf16),
        ),
    )(
        receptance, key_matrix, value_matrix, decay_data_term, correction_rate_data,
        decay_channel_offset.reshape(1, HD), correction_rate_offset.reshape(1, HD), extra_head_log_decay,
    )
    zero = jnp.zeros((HD, HD), f32)
    prefix = entering((dev[:, HD:].astype(f32), dev[:, :HD].astype(f32)), "ep", chain_join, (jnp.eye(HD, dtype=f32), zero))
    mixed_hidden = pl.pallas_call(
        finish_kernel, out_shape=jax.ShapeDtypeStruct((rows, HD), bf16)
    )(out, qp, prefix[1], output_gate_input, head_norm_gain.reshape(1, HD))
    summed = summed_on_arrival(
        jnp.dot(mixed_hidden, mixer_output_weight, preferred_element_type=jnp.float32).astype(
            jnp.bfloat16
        ),
        "tp",
        0,
    )
    return summed.astype(jnp.bfloat16)


def finish_experts(gate_val, up_val, expert_down_weight):
    expert_hidden = (jax.nn.silu(gate_val) * up_val).astype(jnp.bfloat16)
    summed = summed_on_arrival(
        jnp.einsum(
            "sxcf,xfd->dsxc", expert_hidden, expert_down_weight, preferred_element_type=jnp.float32
        ).astype(jnp.bfloat16),
        "tp",
        0,
    )
    return summed.astype(jnp.bfloat16)


def expert_part(
    expert_layer_input,
    feedforward_norm_gain,
    group_router_weight,
    expert_router_weight,
    routes,
    expert_gate_weight,
    expert_up_weight,
    expert_down_weight,
):
    token_rows = expert_layer_input.shape[0]
    route_count = routes.shape[1]
    ep_count = lax.axis_size("ep")
    expert_total = expert_router_weight.shape[1]
    per_group = expert_total // GROUPS
    capacity = 4 * token_rows // ep_count
    widened = expert_layer_input.astype(jnp.float32)
    normed_input = (
        widened
        * lax.rsqrt(jnp.mean(widened * widened, axis=-1, keepdims=True) + norm_eps)
        * feedforward_norm_gain
    ).astype(jnp.bfloat16)
    group_logit = jnp.dot(normed_input, group_router_weight, preferred_element_type=jnp.float32)
    group_exp = jnp.exp(group_logit)
    group_prob = group_exp / jnp.sum(group_exp, axis=-1, keepdims=True)
    expert_logit = jnp.dot(normed_input, expert_router_weight, preferred_element_type=jnp.float32)
    expert_range = jnp.arange(expert_total, dtype=jnp.int32)
    matched = routes[:, :, None] == expert_range[None, None, :]
    chosen_logit = jnp.sum(jnp.where(matched, expert_logit[:, None, :], 0.0), axis=-1)
    group_match = (routes // per_group)[:, :, None] == jnp.arange(GROUPS, dtype=jnp.int32)[
        None, None, :
    ]
    chosen_group = jnp.sum(jnp.where(group_match, group_prob[:, None, :], 0.0), axis=-1)
    route_weight = chosen_group * jax.nn.sigmoid(chosen_logit - chosen_logit[:, ::-1])
    flat_match = matched.reshape(token_rows * route_count, expert_total).astype(jnp.int32)
    before = jnp.cumsum(flat_match, axis=0) - flat_match
    placed = jnp.sum(before * flat_match, axis=1)
    slot_ids = routes.reshape(-1) * capacity + placed
    slot_range = jnp.arange(expert_total * capacity, dtype=jnp.int32)
    struck = (slot_range[:, None] == slot_ids[None, :]).reshape(
        expert_total * capacity, token_rows, route_count
    )
    dispatch_matrix = jnp.any(struck, axis=-1).astype(jnp.bfloat16)
    combine_matrix = jnp.sum(jnp.where(struck, route_weight[None, :, :], 0.0), axis=-1)
    outgoing = jnp.dot(dispatch_matrix, normed_input, preferred_element_type=jnp.float32).astype(
        jnp.bfloat16
    )
    outgoing = outgoing.reshape(ep_count, expert_total // ep_count, capacity, outgoing.shape[1])
    arrived = lax.all_to_all(outgoing, "ep", split_axis=0, concat_axis=0, tiled=True)
    gate_val = jnp.einsum(
        "sxcd,xdf->sxcf", arrived, expert_gate_weight, preferred_element_type=jnp.float32
    )
    up_val = jnp.einsum(
        "sxcd,xdf->sxcf", arrived, expert_up_weight, preferred_element_type=jnp.float32
    )
    expert_rows = finish_experts(gate_val, up_val, expert_down_weight)
    homebound = lax.all_to_all(expert_rows, "ep", split_axis=1, concat_axis=1, tiled=True)
    homebound = homebound.reshape(homebound.shape[0], expert_total * capacity)
    combined = jnp.dot(homebound.astype(jnp.float32), combine_matrix)
    return combined.T.astype(jnp.bfloat16)


def local(
    receptance,
    key_matrix,
    value_matrix,
    decay_data_term,
    correction_rate_data,
    output_gate_input,
    decay_channel_offset,
    correction_rate_offset,
    extra_head_log_decay,
    head_norm_gain,
    mixer_output_weight,
    expert_layer_input,
    feedforward_norm_gain,
    group_router_weight,
    expert_router_weight,
    routes,
    expert_gate_weight,
    expert_up_weight,
    expert_down_weight,
):
    token_mixer_output = mixer_part(
        receptance,
        key_matrix,
        value_matrix,
        decay_data_term,
        correction_rate_data,
        output_gate_input,
        decay_channel_offset,
        correction_rate_offset,
        extra_head_log_decay,
        head_norm_gain,
        mixer_output_weight,
    )
    expert_out = expert_part(
        expert_layer_input,
        feedforward_norm_gain,
        group_router_weight,
        expert_router_weight,
        routes,
        expert_gate_weight,
        expert_up_weight,
        expert_down_weight,
    )
    return (token_mixer_output, expert_out)


def solution(mesh):
    in_specs = (
        P("ep", "tp"),
        P("ep", "tp"),
        P("ep", "tp"),
        P("ep", "tp"),
        P("ep", "tp"),
        P("ep", "tp"),
        P("tp"),
        P("tp"),
        P("ep", "tp"),
        P("tp"),
        P("tp", None),
        P("ep", None),
        P(),
        P(),
        P(),
        P("ep", None),
        P("ep", None, "tp"),
        P("ep", None, "tp"),
        P("ep", "tp", None),
    )
    out_specs = (P(("ep", "tp"), None), P("ep", "tp"))
    return jax.shard_map(local, mesh=mesh, in_specs=in_specs, out_specs=out_specs, check_vma=False)
```

```python
import jax
import jax.numpy as jnp
from jax import lax
from jax.experimental import pallas as pl
from jax.experimental.pallas import tpu as pltpu
from jax.sharding import PartitionSpec as P

f32 = jnp.float32
bf16 = jnp.bfloat16
MESH = pl.DeviceIdType.MESH
HD = 64
CH = 128
NX, NZ, NY = 4, 8, 8
CAP = 16
GROUPS = 4
key_eps = 1e-06
group_eps = 0.00064
norm_eps = 1e-06
HALF = 4
ROWS = 256 // HALF

NN = (((1,), (0,)), ((), ()))
NT = (((1,), (1,)), ((), ()))
TN = (((0,), (0,)), ((), ()))


def dotb(a, b, dims=NN):
    return lax.dot_general(a.astype(bf16), b.astype(bf16), dims, preferred_element_type=f32)


def split(a):
    high = a.astype(bf16)
    return high, (a - high.astype(f32)).astype(bf16)


def dot3(a, b, dims=NN):
    ah, al = split(a)
    bh, bl = split(b)
    return dotb(ah, bh, dims) + (dotb(ah, bl, dims) + dotb(al, bh, dims))


def dot_left2(a, b, dims=NN):
    ah, al = split(a)
    return dotb(ah, b, dims) + dotb(al, b, dims)


def sigmoid(x):
    return 1.0 / (1.0 + jnp.exp(-x))


def iota(shape, dim):
    return lax.broadcasted_iota(jnp.int32, shape, dim)


def column(row):
    n = row.shape[1]
    return jnp.sum(jnp.where(iota((n, n), 0) == iota((n, n), 1), row, 0.0), axis=1, keepdims=True)


def chunk_local(r, k, v, dd, cr, doff, coff, extra):
    C = r.shape[1]
    row, col = iota((C, C), 0), iota((C, C), 1)
    u = k * lax.rsqrt(jnp.sum(k * k, axis=0, keepdims=True) + key_eps)
    a = u * sigmoid(cr + coff)
    lg = extra - 0.6065306597126334 * sigmoid(dd + doff)
    lh, lr = split(lg)
    lm, ll = split(lg - lh.astype(f32))
    tri = jnp.where(row <= col, 1.0, 0.0).astype(bf16)
    cum = dotb(lh, tri) + (dotb(lm, tri) + dotb(ll, tri))
    bef = cum - lg
    tot = cum[:, C - 1 : C]
    ref = 0.5 * tot
    en = jnp.exp(ref - cum)
    lhs = jnp.concatenate([u * jnp.exp(bef - ref), r * jnp.exp(cum - ref)], axis=1)
    rhs = jnp.concatenate([k * en, a * en], axis=1)
    G = dotb(lhs, rhs, TN)
    strict, upto = row > col, row >= col
    kp = jnp.where(strict, G[:C, :C], 0.0)
    A = jnp.where(strict, G[:C, C:], 0.0)
    rk = jnp.where(upto, G[C:, :C], 0.0)
    rr = jnp.where(upto, G[C:, C:], 0.0)
    x = row ^ col
    T = jnp.where(row == col, 1.0, 0.0) - jnp.where(x == 1, A, 0.0)
    s = 2
    while s < C:
        m = jnp.where((x >= s) & (x < 2 * s), A, 0.0)
        T = T - dot3(T, dot3(m, T))
        s *= 2
    R = jnp.concatenate([dotb(v, kp, NT), u * jnp.exp(bef)], axis=0)
    X = dotb(R, T, NT)
    out = jnp.concatenate([dotb(v, rk, NT), r * jnp.exp(cum)], axis=0) - dotb(X, rr, NT)
    tail = jnp.exp(tot - cum)
    diag = jnp.where(iota((HD, HD), 0) == iota((HD, HD), 1), jnp.exp(tot), 0.0)
    bm = jnp.concatenate([dotb(v, k * tail, NT), diag], axis=0) - dotb(X, a * tail, NT)
    return out, bm


def whole(
    rT, kT, vT, ddT, crT, gateT, doff, coff, extraT, gain, wmix, xin, fgain, grw, erw, routes,
    wg_hbm, wu_hbm, wd_hbm, wmix_hbm,
    tmo, eo,
    wg, wu, wd, wmp, wload, wsend, wrecv,
    dbuf, X, wch, wcl, dsp_s, dsp_r, ag_s, ag_r,
    outT, qp, xg, xg_s, xg_r, zg, ztot, zg_s, zg_r,
    mx, mxp, mx_s, mx_r, pm, msb, mrb, ms_s, ms_r,
    hid, epm, esb, erb, es_s, es_r, res, home, rt_s, rt_r,
):
    ep, tp = lax.axis_index("ep"), lax.axis_index("tp")
    y, c = tp // 2, tp % 2
    z, x = ep // NX, ep % NX
    half, seat = ep // 16, ep % 16
    partner = (ep, tp + 1 - 2 * c)

    def rdma(src, dst, ssem, rsem, device):
        return pltpu.make_async_remote_copy(
            src_ref=src, dst_ref=dst, send_sem=ssem, recv_sem=rsem, device_id=device, device_id_type=MESH
        )

    def got(ref, sem):
        rdma(ref, ref, sem, sem, partner).wait_recv()

    def sent(ref, sem):
        rdma(ref, ref, sem, sem, partner).wait_send()

    barrier = pltpu.get_barrier_semaphore()

    def greet(device):
        pl.semaphore_signal(barrier, inc=1, device_id=device, device_id_type=MESH)

    def meet(e, _):
        @pl.when(jnp.logical_not((e == ep) & (half == c)))
        def _():
            greet((e, 2 * y + half))

        there, cc = c * 16 + e // 2, e % 2

        @pl.when(jnp.logical_not((there == ep) & (cc == c)))
        def _():
            greet((there, 2 * y + cc))

        return 0

    lax.fori_loop(0, 32, meet, 0)
    greet(partner)
    for d in (1, NY - 1):
        greet((ep, 2 * ((y + d) % NY) + c))
    for d in range(1, NX):
        greet((z * NX + (x + d) % NX, tp))
    for d in range(1, NZ):
        greet(((z + d) % NZ * NX + x, tp))

    loads, swaps = [], []
    for n, (hbm, dst) in enumerate(((wg_hbm, wg), (wu_hbm, wu))):
        for q in range(2):
            loads.append(pltpu.make_async_copy(hbm.at[q], dst.at[0, :, :, q], wload.at[2 * n + q]))
            swaps.append(rdma(hbm.at[q], dst.at[1, :, :, q], wsend.at[2 * n + q], wrecv.at[2 * n + q], partner))
    loads.append(pltpu.make_async_copy(wd_hbm, wd.at[0], wload.at[4]))
    swaps.append(rdma(wd_hbm, wd.at[1], wsend.at[4], wrecv.at[4], partner))
    swaps.append(rdma(wmix_hbm, wmp, wsend.at[5], wrecv.at[5], partner))
    for copy in loads:
        copy.start()

    xf = xin[...].astype(f32)
    rs = lax.rsqrt(jnp.mean(xf * xf, axis=-1, keepdims=True) + norm_eps)
    r0, r1 = routes[0:1, :], routes[1:2, :]
    experts = iota((32, 128), 0)
    m0 = jnp.where(r0 == experts, 1.0, 0.0)
    m1 = jnp.where(r1 == experts, 1.0, 0.0)
    before = jnp.where(iota((128, 128), 0) < iota((128, 128), 1), 1.0, 0.0)
    rank = dotb(m0 + m1, before)
    spread = jnp.where(iota((512, 32), 0) // CAP == iota((512, 32), 1), 1.0, 0.0)
    placed = jnp.where(dotb(spread, rank) == (iota((512, 128), 0) % CAP).astype(f32), dotb(spread, m0 + m1), 0.0)
    fours = y % 4
    for q in range(2):
        cols = pl.ds(pl.multiple_of((2 * fours + 8 * q + c) * 128, 128), 128)
        mine = (xin[:, cols].astype(f32) * rs * fgain[:, cols]).astype(bf16)
        dbuf[:, q * 128 : (q + 1) * 128] = dotb(placed, mine).astype(bf16)

    def dispatch(e, _):
        src = dbuf.at[pl.ds(pl.multiple_of(e * CAP, CAP), CAP), :]
        dst = X.at[
            pl.ds(pl.multiple_of(seat * CAP, CAP), CAP), pl.ds(pl.multiple_of(fours * 512 + c * 256, 128), 256)
        ]
        here = (e == ep) & (half == c)

        @pl.when(here)
        def _():
            pltpu.make_async_copy(src, dst, dsp_r).start()

        @pl.when(jnp.logical_not(here))
        def _():
            rdma(src, dst, dsp_s, dsp_r, (e, 2 * y + half)).start()

        return 0

    def length(d, h):
        return 4 if d == h % 2 else 3

    def at_y(v):
        return (v + 2 * NY) % NY

    def neighbour(d):
        return (ep, 2 * at_y(y + 1 - 2 * d) + c)

    def lanes(s):
        return pl.ds(pl.multiple_of(s * 256, 256), 256)

    def ag_block(place, h):
        return X.at[h * ROWS : (h + 1) * ROWS, pl.ds(pl.multiple_of(at_y(place) % 4 * 512, 512), 512)]

    def behind(d):
        return y - 1 if d == 0 else y + 1

    def ag_copy(d, h, s):
        ref = ag_block(y if s == 0 else behind(d), h)
        return rdma(ref, ref, ag_s.at[d, h, s], ag_r.at[d, h, s], neighbour(d))

    def ag_first():
        for h in range(HALF):
            for d in (h % 2, 1 - h % 2):
                ag_copy(d, h, 0).start()

    def ag_second():
        for h in range(HALF):
            for d in (h % 2, 1 - h % 2):
                got(ag_block(behind(d), h), ag_r.at[d, h, 0])
                if h % 2 == d:
                    ag_copy(d, h, 1).start()

    def ag_done():
        for h in range(HALF):
            got(ag_block(y + 2, h), ag_r.at[h % 2, h, 1])

    def local_chunk(n):
        sl = slice(n * CH, (n + 1) * CH)
        out, bm = chunk_local(
            rT[:, sl].astype(f32), kT[:, sl].astype(f32), vT[:, sl].astype(f32), ddT[:, sl].astype(f32),
            crT[:, sl].astype(f32), column(doff[...]), column(coff[...]), extraT[:, sl],
        )
        outT[n] = out
        return bm

    upper = iota((2 * HD, HD), 0)
    across = iota((2 * HD, HD), 1)

    def join(stack, later_q, later_p):
        return dot_left2(stack, later_p) + jnp.concatenate([later_q, jnp.zeros((HD, HD), f32)], axis=0)

    def rs_step(s, part, sbuf, rbuf, ssem, rsem):
        for h in range(HALF):
            for d in range(2):
                n = length(d, h)
                if s >= n:
                    continue
                dest = at_y(y + (n - s) if d == 0 else y - (n - s))
                value = part(dest, h)
                if s > 0:
                    got(rbuf.at[d, h, s - 1], rsem.at[d, h, s - 1])
                    value = value + rbuf[d, h, s - 1].astype(f32)
                sbuf[d, h, s] = value.astype(bf16)
                rdma(sbuf.at[d, h, s], rbuf.at[d, h, s], ssem.at[d, h, s], rsem.at[d, h, s], neighbour(d)).start()

    def rs_last(h, part, rbuf, rsem):
        value = part(y, h)
        for d in range(2):
            n = length(d, h) - 1
            got(rbuf.at[d, h, n], rsem.at[d, h, n])
            value = value + rbuf[d, h, n].astype(f32)
        return value

    def mix_part(dest, h):
        return pm[dest, :, h * (2048 // HALF) : (h + 1) * (2048 // HALF)]

    @pl.when(half == c)
    def _():
        pl.semaphore_wait(barrier, 62 + 3 + NX - 1 + NZ - 1)

    @pl.when(half != c)
    def _():
        pl.semaphore_wait(barrier, 64 + 3 + NX - 1 + NZ - 1)

    lax.fori_loop(0, 32, dispatch, 0)
    for copy in swaps:
        copy.start()

    bms = [local_chunk(n) for n in range(2)]
    got(X.at[:, pl.ds(pl.multiple_of(fours * 512, 512), 512)], dsp_r)
    ag_first()
    bms += [local_chunk(n) for n in range(2, 4)]
    stack = jnp.where(upper == across + HD, 1.0, 0.0)
    for n in range(4):
        qp[n] = stack
        stack = dot3(stack, bms[n][HD:]) + jnp.where(upper < HD, bms[n], 0.0)
    xg[0] = jnp.concatenate([stack[:HD], stack[HD:]], axis=1).astype(bf16)
    x_copies = []
    for rr in range(1, NX):
        to = (z * NX + (x + rr) % NX, tp)
        x_copies.append(rdma(xg.at[0], xg.at[rr], xg_s.at[rr], xg_r.at[rr], to))
        x_copies[-1].start()

    ag_second()
    for rr in range(1, NX):
        got(xg.at[rr], xg_r.at[rr])
    stack = jnp.where(upper == across + HD, 1.0, 0.0)
    own_q, own_p = jnp.zeros((HD, HD), f32), jnp.zeros((HD, HD), f32)
    for i in range(NX):
        own_q = jnp.where(x == i, stack[:HD], own_q)
        own_p = jnp.where(x == i, stack[HD:], own_p)
        piece = xg[(x - i + NX) % NX].astype(f32)
        stack = join(stack, piece[:, :HD], piece[:, HD:])
    ztot[...] = jnp.concatenate([stack[:HD], stack[HD:]], axis=1).astype(bf16)
    for rr in range(1, NZ):

        @pl.when(z + rr < NZ)
        def _():
            rdma(ztot, zg.at[z], zg_s.at[rr], zg_r.at[z], ((z + rr) * NX + x, tp)).start()

    nb = (xf * rs * fgain[...]).astype(bf16)
    logit = dotb(erw[...], nb, NT)
    gexp = jnp.exp(dotb(grw[...], nb, NT))
    gprob = gexp / jnp.sum(gexp, axis=0, keepdims=True)
    c0 = jnp.sum(jnp.where(r0 == experts, logit, 0.0), axis=0, keepdims=True)
    c1 = jnp.sum(jnp.where(r1 == experts, logit, 0.0), axis=0, keepdims=True)
    groups = iota((GROUPS, 128), 0)
    g0 = jnp.sum(jnp.where(r0 // 8 == groups, gprob, 0.0), axis=0, keepdims=True)
    g1 = jnp.sum(jnp.where(r1 // 8 == groups, gprob, 0.0), axis=0, keepdims=True)
    weight = m0 * (g0 * sigmoid(c0 - c1)) + m1 * (g1 * sigmoid(c1 - c0))
    wh, wl = split(weight)
    full = placed * (dotb(spread, wh) + dotb(spread, wl))
    fh, fl = split(full.T)
    wch[...] = fh
    wcl[...] = fl

    ag_done()
    for copy in loads:
        copy.wait()
    for copy in swaps[:5]:
        copy.wait_recv()
    for q in range(2):
        g = dotb(X[...], wg[q].reshape(2048, 256))
        u = dotb(X[...], wu[q].reshape(2048, 256))
        hid[:, q * 256 : (q + 1) * 256] = (g * sigmoid(g) * u).astype(bf16)

    def down(shift):
        dest = at_y(y + shift)
        epm[dest] = dotb(hid[:, :256], wd[0, :, lanes(dest)]) + dotb(hid[:, 256:], wd[1, :, lanes(dest)])

    def exp_part(dest, h):
        return epm[dest, h * ROWS : (h + 1) * ROWS]

    for shift in (4, 3, -3):
        down(shift)
    rs_step(0, exp_part, esb, erb, es_s, es_r)
    def fold(i, state):
        got(zg.at[i], zg_r.at[i])
        piece = zg[i].astype(f32)
        return dot_left2(state, piece[:, HD:]) + piece[:, :HD]

    state = lax.fori_loop(0, z, fold, jnp.zeros((HD, HD), f32))
    state = dot3(state, own_p) + own_q
    gain_c = column(gain[...])
    for n in range(4):
        sl = slice(n * CH, (n + 1) * CH)
        q = qp[n]
        now = dot3(state, q[HD:]) + q[:HD]
        o = outT[n]
        ho = o[:HD] + dotb(now, o[HD:])
        ho = ho - jnp.mean(ho, axis=0, keepdims=True)
        sp = jnp.mean(ho * ho, axis=0, keepdims=True)
        mixed = ho * lax.rsqrt(sp + group_eps) * gain_c * sigmoid(gateT[:, sl].astype(f32))
        mx[2 * n : 2 * n + 2] = mixed.T.reshape(2, 2, 32, HD).astype(bf16)
    pair = rdma(mx.at[:, 1 - c], mxp, mx_s, mx_r, partner)
    pair.start()
    for shift in (2, -2):
        down(shift)
    rs_step(1, exp_part, esb, erb, es_s, es_r)
    pair.wait_recv()
    swaps[5].wait_recv()
    total = dotb(mx[:, c].reshape(256, HD), wmix[...]) + dotb(mxp[...].reshape(256, HD), wmp[...])
    pm[...] = total.reshape(NY, 32, 2048)

    rs_step(0, mix_part, msb, mrb, ms_s, ms_r)
    for shift in (1, -1, 0):
        down(shift)
    rs_step(2, exp_part, esb, erb, es_s, es_r)
    rs_step(1, mix_part, msb, mrb, ms_s, ms_r)
    rs_step(3, exp_part, esb, erb, es_s, es_r)
    def send_home(n, _):
        j, cc = n // 2, n % 2
        src = res.at[pl.ds(pl.multiple_of(j * CAP, CAP), CAP), pl.ds(pl.multiple_of(cc * 128, 128), 128)]
        dst = home.at[pl.ds(pl.multiple_of(ep * CAP, CAP), CAP), :]
        there = c * 16 + j
        here = (there == ep) & (cc == c)

        @pl.when(here)
        def _():
            pltpu.make_async_copy(src, dst, rt_r).start()

        @pl.when(jnp.logical_not(here))
        def _():
            rdma(src, dst, rt_s, rt_r, (there, 2 * y + cc)).start()

        return 0

    for h in range(HALF):
        res[h * ROWS : (h + 1) * ROWS] = rs_last(h, exp_part, erb, es_r).astype(bf16)
        lax.fori_loop(h * (32 // HALF), (h + 1) * (32 // HALF), send_home, 0)

    rs_step(2, mix_part, msb, mrb, ms_s, ms_r)
    rs_step(3, mix_part, msb, mrb, ms_s, ms_r)
    for h in range(HALF):
        tmo[:, h * (2048 // HALF) : (h + 1) * (2048 // HALF)] = rs_last(h, mix_part, mrb, ms_r).astype(bf16)
    got(home, rt_r)
    eo[...] = (dotb(wch[...], home[...]) + dotb(wcl[...], home[...])).astype(bf16)

    for copy in swaps:
        copy.wait_send()
    for copy in x_copies:
        copy.wait_send()
    for rr in range(1, NZ):

        @pl.when(z + rr < NZ)
        def _():
            sent(ztot, zg_s.at[rr])

    pair.wait_send()

    @pl.when(half == c)
    def _():
        sent(dbuf.at[0:496], dsp_s)
        sent(home.at[0:496], rt_s)

    @pl.when(half != c)
    def _():
        sent(dbuf, dsp_s)
        sent(home, rt_s)

    for d in range(2):
        for h in range(HALF):
            for s in range(length(d, h)):
                if s == 0 or (s == 1 and h % 2 == d):
                    ag_copy(d, h, s).wait_send()
                sent(msb.at[d, h, s], ms_s.at[d, h, s])
                sent(esb.at[d, h, s], es_s.at[d, h, s])


def local(
    receptance, key_matrix, value_matrix, decay_data_term, correction_rate_data, output_gate_input,
    decay_channel_offset, correction_rate_offset, extra_head_log_decay, head_norm_gain, mixer_output_weight,
    expert_layer_input, feedforward_norm_gain, group_router_weight, expert_router_weight, routes,
    expert_gate_weight, expert_up_weight, expert_down_weight,
):
    V = pltpu.VMEM
    DMA = pltpu.SemaphoreType.DMA
    ring = (2, HALF, 4)
    vm = pl.BlockSpec(memory_space=pltpu.VMEM)
    anyw = pl.BlockSpec(memory_space=pl.ANY)
    return pl.pallas_call(
        whole,
        out_shape=(
            jax.ShapeDtypeStruct((32, 2048), bf16),
            jax.ShapeDtypeStruct((128, 128), bf16),
        ),
        in_specs=[vm] * 16 + [anyw] * 4,
        out_specs=(vm, vm),
        scratch_shapes=[
            V((2, 4, 2, 2, 128, 256), bf16), V((2, 4, 2, 2, 128, 256), bf16), V((2, 256, 2048), bf16), V((HD, 2048), bf16),
            DMA((5,)), DMA((6,)), DMA((6,)),
            V((512, 256), bf16), V((256, 2048), bf16), V((128, 512), bf16), V((128, 512), bf16), DMA, DMA, DMA(ring), DMA(ring),
            V((4, 2 * HD, CH), f32), V((4, 2 * HD, HD), f32), V((NX, HD, 2 * HD), bf16), DMA((NX,)), DMA((NX,)),
            V((NZ, HD, 2 * HD), bf16), V((HD, 2 * HD), bf16), DMA((NZ,)), DMA((NZ,)),
            V((NY, 2, 32, HD), bf16), V((NY, 32, HD), bf16), DMA, DMA, V((NY, 32, 2048), f32),
            V((*ring, 32, 2048 // HALF), bf16), V((*ring, 32, 2048 // HALF), bf16), DMA(ring), DMA(ring),
            V((256, 512), bf16), V((NY, 256, 256), f32), V((*ring, ROWS, 256), bf16), V((*ring, ROWS, 256), bf16), DMA(ring), DMA(ring),
            V((256, 256), bf16), V((512, 128), bf16), DMA, DMA,
        ],
        compiler_params=pltpu.CompilerParams(has_side_effects=True, collective_id=0, vmem_limit_bytes=60000 * 1024),
    )(
        receptance.T, key_matrix.T, value_matrix.T, decay_data_term.T, correction_rate_data.T, output_gate_input.T,
        decay_channel_offset.reshape(1, HD), correction_rate_offset.reshape(1, HD), extra_head_log_decay.T,
        head_norm_gain.reshape(1, HD), mixer_output_weight, expert_layer_input, feedforward_norm_gain.reshape(1, 2048),
        group_router_weight.T, expert_router_weight.T, routes.T,
        expert_gate_weight.reshape(2, 4, 2, 128, 256), expert_up_weight.reshape(2, 4, 2, 128, 256), expert_down_weight[0], mixer_output_weight,
    )


def solution(mesh):
    in_specs = (
        P("ep", "tp"), P("ep", "tp"), P("ep", "tp"), P("ep", "tp"), P("ep", "tp"), P("ep", "tp"),
        P("tp"), P("tp"), P("ep", "tp"), P("tp"), P("tp", None),
        P("ep", None), P(), P(), P(), P("ep", None),
        P("ep", None, "tp"), P("ep", None, "tp"), P("ep", "tp", None),
    )
    out_specs = (P(("ep", "tp"), None), P("ep", "tp"))
    return jax.shard_map(local, mesh=mesh, in_specs=in_specs, out_specs=out_specs, check_vma=False)
```

```python
import jax
import jax.numpy as jnp
from jax import lax
from jax.experimental import pallas as pl
from jax.experimental.pallas import tpu as pltpu
from jax.sharding import PartitionSpec as P

f32 = jnp.float32
bf16 = jnp.bfloat16
MESH = pl.DeviceIdType.MESH
HD = 64
CH = 128
NX, NZ, NY = 4, 8, 8
CAP = 16
GROUPS = 4
key_eps = 1e-06
group_eps = 0.00064
norm_eps = 1e-06
HALF = 4
ROWS = 256 // HALF

NN = (((1,), (0,)), ((), ()))
NT = (((1,), (1,)), ((), ()))
TN = (((0,), (0,)), ((), ()))


def dotb(a, b, dims=NN):
    return lax.dot_general(a.astype(bf16), b.astype(bf16), dims, preferred_element_type=f32)


def split(a):
    high = a.astype(bf16)
    return high, (a - high.astype(f32)).astype(bf16)


def dot3(a, b, dims=NN):
    ah, al = split(a)
    bh, bl = split(b)
    return dotb(ah, bh, dims) + (dotb(ah, bl, dims) + dotb(al, bh, dims))


def dot_left2(a, b, dims=NN):
    ah, al = split(a)
    return dotb(ah, b, dims) + dotb(al, b, dims)


def sigmoid(x):
    return 1.0 / (1.0 + jnp.exp(-x))


def iota(shape, dim):
    return lax.broadcasted_iota(jnp.int32, shape, dim)


def column(row):
    n = row.shape[1]
    return jnp.sum(jnp.where(iota((n, n), 0) == iota((n, n), 1), row, 0.0), axis=1, keepdims=True)


def chunk_pairs(r, k, v, dd, cr, doff, coff, extra):
    C = r.shape[1]
    row, col = iota((C, C), 0), iota((C, C), 1)
    u = k * lax.rsqrt(jnp.sum(k * k, axis=0, keepdims=True) + key_eps)
    a = u * sigmoid(cr + coff)
    lg = extra - 0.6065306597126334 * sigmoid(dd + doff)
    lh, lr = split(lg)
    lm, ll = split(lg - lh.astype(f32))
    tri = jnp.where(row <= col, 1.0, 0.0).astype(bf16)
    cum = dotb(lh, tri) + (dotb(lm, tri) + dotb(ll, tri))
    bef = cum - lg
    tot = cum[:, C - 1 : C]
    ref = 0.5 * tot
    en = jnp.exp(ref - cum)
    lhs = jnp.concatenate([u * jnp.exp(bef - ref), r * jnp.exp(cum - ref)], axis=1)
    rhs = jnp.concatenate([k * en, a * en], axis=1)
    G = dotb(lhs, rhs, TN)
    strict, upto = row > col, row >= col
    kp = jnp.where(strict, G[:C, :C], 0.0)
    A = jnp.where(strict, G[:C, C:], 0.0)
    rk = jnp.where(upto, G[C:, :C], 0.0)
    rr = jnp.where(upto, G[C:, C:], 0.0)
    R = jnp.concatenate([dotb(v, kp, NT), u * jnp.exp(bef)], axis=0)
    out = jnp.concatenate([dotb(v, rk, NT), r * jnp.exp(cum)], axis=0)
    tail = jnp.exp(tot - cum)
    diag = jnp.where(iota((HD, HD), 0) == iota((HD, HD), 1), jnp.exp(tot), 0.0)
    bm = jnp.concatenate([dotb(v, k * tail, NT), diag], axis=0)
    return A, R, out, rr, bm, a * tail


def inverses(pairs):
    C = pairs[0].shape[0]
    x = iota((C, C), 0) ^ iota((C, C), 1)
    found = [jnp.where(x == 0, 1.0, 0.0) - jnp.where(x == 1, A, 0.0) for A in pairs]
    s = 2
    while s < C:
        level = (x >= s) & (x < 2 * s)
        right = [dot3(jnp.where(level, A, 0.0), T) for A, T in zip(pairs, found)]
        found = [T - dot3(T, m) for T, m in zip(found, right)]
        s *= 2
    return found


def chunk_ends(T, R, out, rr, bm, at):
    X = dotb(R, T, NT)
    return out - dotb(X, rr, NT), bm - dotb(X, at, NT)


def whole(
    rT, kT, vT, ddT, crT, gateT, doff, coff, extraT, gain, wmix, xin, fgain, grw, erw, routes,
    wg_hbm, wu_hbm, wd_hbm, wmix_hbm,
    tmo, eo,
    wg, wu, wd, wmp, wload, wsend, wrecv,
    dbuf, X, wch, wcl, dsp_s, dsp_r, ag_s, ag_r,
    outT, qp, xg, xg_s, xg_r, zg, ztot, zg_s, zg_r,
    mx, mxp, mx_s, mx_r, pm, msb, mrb, ms_s, ms_r,
    hid, epm, esb, erb, es_s, es_r, res, home, rt_s, rt_r,
):
    ep, tp = lax.axis_index("ep"), lax.axis_index("tp")
    y, c = tp // 2, tp % 2
    z, x = ep // NX, ep % NX
    half, seat = ep // 16, ep % 16
    partner = (ep, tp + 1 - 2 * c)

    def rdma(src, dst, ssem, rsem, device):
        return pltpu.make_async_remote_copy(
            src_ref=src, dst_ref=dst, send_sem=ssem, recv_sem=rsem, device_id=device, device_id_type=MESH
        )

    def got(ref, sem):
        rdma(ref, ref, sem, sem, partner).wait_recv()

    def sent(ref, sem):
        rdma(ref, ref, sem, sem, partner).wait_send()

    barrier = pltpu.get_barrier_semaphore()

    def greet(device):
        pl.semaphore_signal(barrier, inc=1, device_id=device, device_id_type=MESH)

    def meet(e, _):
        @pl.when(jnp.logical_not((e == ep) & (half == c)))
        def _():
            greet((e, 2 * y + half))

        there, cc = c * 16 + e // 2, e % 2

        @pl.when(jnp.logical_not((there == ep) & (cc == c)))
        def _():
            greet((there, 2 * y + cc))

        return 0

    lax.fori_loop(0, 32, meet, 0)
    greet(partner)
    for d in (1, NY - 1):
        greet((ep, 2 * ((y + d) % NY) + c))
    for d in range(1, NX):
        greet((z * NX + (x + d) % NX, tp))
    for d in range(1, NZ):
        greet(((z + d) % NZ * NX + x, tp))

    loads, swaps = [], []
    for n, (hbm, dst) in enumerate(((wg_hbm, wg), (wu_hbm, wu))):
        for q in range(2):
            loads.append(pltpu.make_async_copy(hbm.at[q], dst.at[0, :, :, q], wload.at[2 * n + q]))
            swaps.append(rdma(hbm.at[q], dst.at[1, :, :, q], wsend.at[2 * n + q], wrecv.at[2 * n + q], partner))
    loads.append(pltpu.make_async_copy(wd_hbm, wd.at[0], wload.at[4]))
    swaps.append(rdma(wd_hbm, wd.at[1], wsend.at[4], wrecv.at[4], partner))
    swaps.append(rdma(wmix_hbm, wmp, wsend.at[5], wrecv.at[5], partner))
    for copy in loads:
        copy.start()

    xf = xin[...].astype(f32)
    rs = lax.rsqrt(jnp.mean(xf * xf, axis=-1, keepdims=True) + norm_eps)
    r0, r1 = routes[0:1, :], routes[1:2, :]
    experts = iota((32, 128), 0)
    m0 = jnp.where(r0 == experts, 1.0, 0.0)
    m1 = jnp.where(r1 == experts, 1.0, 0.0)
    before = jnp.where(iota((128, 128), 0) < iota((128, 128), 1), 1.0, 0.0)
    rank = dotb(m0 + m1, before)
    spread = jnp.where(iota((512, 32), 0) // CAP == iota((512, 32), 1), 1.0, 0.0)
    placed = jnp.where(dotb(spread, rank) == (iota((512, 128), 0) % CAP).astype(f32), dotb(spread, m0 + m1), 0.0)
    fours = y % 4
    for q in range(2):
        cols = pl.ds(pl.multiple_of((2 * fours + 8 * q + c) * 128, 128), 128)
        mine = (xin[:, cols].astype(f32) * rs * fgain[:, cols]).astype(bf16)
        dbuf[:, q * 128 : (q + 1) * 128] = dotb(placed, mine).astype(bf16)

    def dispatch(e, _):
        src = dbuf.at[pl.ds(pl.multiple_of(e * CAP, CAP), CAP), :]
        dst = X.at[
            pl.ds(pl.multiple_of(seat * CAP, CAP), CAP), pl.ds(pl.multiple_of(fours * 512 + c * 256, 128), 256)
        ]
        here = (e == ep) & (half == c)

        @pl.when(here)
        def _():
            pltpu.make_async_copy(src, dst, dsp_r).start()

        @pl.when(jnp.logical_not(here))
        def _():
            rdma(src, dst, dsp_s, dsp_r, (e, 2 * y + half)).start()

        return 0

    def length(d, h):
        return 4 if d == h % 2 else 3

    def at_y(v):
        return (v + 2 * NY) % NY

    def neighbour(d):
        return (ep, 2 * at_y(y + 1 - 2 * d) + c)

    def lanes(s):
        return pl.ds(pl.multiple_of(s * 256, 256), 256)

    def ag_block(place, h):
        return X.at[h * ROWS : (h + 1) * ROWS, pl.ds(pl.multiple_of(at_y(place) % 4 * 512, 512), 512)]

    def behind(d):
        return y - 1 if d == 0 else y + 1

    def ag_copy(d, h, s):
        ref = ag_block(y if s == 0 else behind(d), h)
        return rdma(ref, ref, ag_s.at[d, h, s], ag_r.at[d, h, s], neighbour(d))

    def ag_first():
        for h in range(HALF):
            for d in (h % 2, 1 - h % 2):
                ag_copy(d, h, 0).start()

    def ag_second():
        for h in range(HALF):
            for d in (h % 2, 1 - h % 2):
                got(ag_block(behind(d), h), ag_r.at[d, h, 0])
                if h % 2 == d:
                    ag_copy(d, h, 1).start()

    def ag_done():
        for h in range(HALF):
            got(ag_block(y + 2, h), ag_r.at[h % 2, h, 1])

    def local_chunks(numbers):
        pairs = []
        for n in numbers:
            sl = slice(n * CH, (n + 1) * CH)
            pairs.append(
                chunk_pairs(
                    rT[:, sl].astype(f32), kT[:, sl].astype(f32), vT[:, sl].astype(f32), ddT[:, sl].astype(f32),
                    crT[:, sl].astype(f32), column(doff[...]), column(coff[...]), extraT[:, sl],
                )
            )
        bms = []
        for n, T, p in zip(numbers, inverses([p[0] for p in pairs]), pairs):
            outT[n], bm = chunk_ends(T, *p[1:])
            bms.append(bm)
        return bms

    upper = iota((2 * HD, HD), 0)
    across = iota((2 * HD, HD), 1)

    def join(stack, later_q, later_p):
        return dot_left2(stack, later_p) + jnp.concatenate([later_q, jnp.zeros((HD, HD), f32)], axis=0)

    def rs_step(s, part, sbuf, rbuf, ssem, rsem):
        for h in range(HALF):
            for d in range(2):
                n = length(d, h)
                if s >= n:
                    continue
                dest = at_y(y + (n - s) if d == 0 else y - (n - s))
                value = part(dest, h)
                if s > 0:
                    got(rbuf.at[d, h, s - 1], rsem.at[d, h, s - 1])
                    value = value + rbuf[d, h, s - 1].astype(f32)
                sbuf[d, h, s] = value.astype(bf16)
                rdma(sbuf.at[d, h, s], rbuf.at[d, h, s], ssem.at[d, h, s], rsem.at[d, h, s], neighbour(d)).start()

    def rs_last(h, part, rbuf, rsem):
        value = part(y, h)
        for d in range(2):
            n = length(d, h) - 1
            got(rbuf.at[d, h, n], rsem.at[d, h, n])
            value = value + rbuf[d, h, n].astype(f32)
        return value

    def mix_part(dest, h):
        return pm[dest, :, h * (2048 // HALF) : (h + 1) * (2048 // HALF)]

    @pl.when(half == c)
    def _():
        pl.semaphore_wait(barrier, 62 + 3 + NX - 1 + NZ - 1)

    @pl.when(half != c)
    def _():
        pl.semaphore_wait(barrier, 64 + 3 + NX - 1 + NZ - 1)

    lax.fori_loop(0, 32, dispatch, 0)
    for copy in swaps:
        copy.start()

    bms = local_chunks((0, 1, 2, 3))
    stack = jnp.where(upper == across + HD, 1.0, 0.0)
    for n in range(4):
        qp[n] = stack
        stack = dot3(stack, bms[n][HD:]) + jnp.where(upper < HD, bms[n], 0.0)
    xg[0] = jnp.concatenate([stack[:HD], stack[HD:]], axis=1).astype(bf16)
    x_copies = []
    for rr in range(1, NX):
        to = (z * NX + (x + rr) % NX, tp)
        x_copies.append(rdma(xg.at[0], xg.at[rr], xg_s.at[rr], xg_r.at[rr], to))
        x_copies[-1].start()

    got(X.at[:, pl.ds(pl.multiple_of(fours * 512, 512), 512)], dsp_r)
    ag_first()
    for rr in range(1, NX):
        got(xg.at[rr], xg_r.at[rr])
    stack = jnp.where(upper == across + HD, 1.0, 0.0)
    own_q, own_p = jnp.zeros((HD, HD), f32), jnp.zeros((HD, HD), f32)
    for i in range(NX):
        own_q = jnp.where(x == i, stack[:HD], own_q)
        own_p = jnp.where(x == i, stack[HD:], own_p)
        piece = xg[(x - i + NX) % NX].astype(f32)
        stack = join(stack, piece[:, :HD], piece[:, HD:])
    ztot[...] = jnp.concatenate([stack[:HD], stack[HD:]], axis=1).astype(bf16)
    for rr in range(1, NZ):

        @pl.when(z + rr < NZ)
        def _():
            rdma(ztot, zg.at[z], zg_s.at[rr], zg_r.at[z], ((z + rr) * NX + x, tp)).start()

    ag_second()
    nb = (xf * rs * fgain[...]).astype(bf16)
    logit = dotb(erw[...], nb, NT)
    gexp = jnp.exp(dotb(grw[...], nb, NT))
    gprob = gexp / jnp.sum(gexp, axis=0, keepdims=True)
    c0 = jnp.sum(jnp.where(r0 == experts, logit, 0.0), axis=0, keepdims=True)
    c1 = jnp.sum(jnp.where(r1 == experts, logit, 0.0), axis=0, keepdims=True)
    groups = iota((GROUPS, 128), 0)
    g0 = jnp.sum(jnp.where(r0 // 8 == groups, gprob, 0.0), axis=0, keepdims=True)
    g1 = jnp.sum(jnp.where(r1 // 8 == groups, gprob, 0.0), axis=0, keepdims=True)
    weight = m0 * (g0 * sigmoid(c0 - c1)) + m1 * (g1 * sigmoid(c1 - c0))
    wh, wl = split(weight)
    full = placed * (dotb(spread, wh) + dotb(spread, wl))
    fh, fl = split(full.T)
    wch[...] = fh
    wcl[...] = fl

    ag_done()
    for copy in loads:
        copy.wait()
    for copy in swaps[:5]:
        copy.wait_recv()
    for q in range(2):
        g = dotb(X[...], wg[q].reshape(2048, 256))
        u = dotb(X[...], wu[q].reshape(2048, 256))
        hid[:, q * 256 : (q + 1) * 256] = (g * sigmoid(g) * u).astype(bf16)

    def down(shift):
        dest = at_y(y + shift)
        epm[dest] = dotb(hid[:, :256], wd[0, :, lanes(dest)]) + dotb(hid[:, 256:], wd[1, :, lanes(dest)])

    def exp_part(dest, h):
        return epm[dest, h * ROWS : (h + 1) * ROWS]

    for shift in (4, 3, -3):
        down(shift)
    rs_step(0, exp_part, esb, erb, es_s, es_r)
    def fold(i, state):
        got(zg.at[i], zg_r.at[i])
        piece = zg[i].astype(f32)
        return dot_left2(state, piece[:, HD:]) + piece[:, :HD]

    state = lax.fori_loop(0, z, fold, jnp.zeros((HD, HD), f32))
    state = dot3(state, own_p) + own_q
    gain_c = column(gain[...])
    for n in range(4):
        sl = slice(n * CH, (n + 1) * CH)
        q = qp[n]
        now = dot3(state, q[HD:]) + q[:HD]
        o = outT[n]
        ho = o[:HD] + dotb(now, o[HD:])
        ho = ho - jnp.mean(ho, axis=0, keepdims=True)
        sp = jnp.mean(ho * ho, axis=0, keepdims=True)
        mixed = ho * lax.rsqrt(sp + group_eps) * gain_c * sigmoid(gateT[:, sl].astype(f32))
        mx[2 * n : 2 * n + 2] = mixed.T.reshape(2, 2, 32, HD).astype(bf16)
    pair = rdma(mx.at[:, 1 - c], mxp, mx_s, mx_r, partner)
    pair.start()
    for shift in (2, -2):
        down(shift)
    rs_step(1, exp_part, esb, erb, es_s, es_r)
    pair.wait_recv()
    swaps[5].wait_recv()
    total = dotb(mx[:, c].reshape(256, HD), wmix[...]) + dotb(mxp[...].reshape(256, HD), wmp[...])
    pm[...] = total.reshape(NY, 32, 2048)

    rs_step(0, mix_part, msb, mrb, ms_s, ms_r)
    for shift in (1, -1, 0):
        down(shift)
    rs_step(2, exp_part, esb, erb, es_s, es_r)
    rs_step(1, mix_part, msb, mrb, ms_s, ms_r)
    rs_step(3, exp_part, esb, erb, es_s, es_r)
    def send_home(n, _):
        j, cc = n // 2, n % 2
        src = res.at[pl.ds(pl.multiple_of(j * CAP, CAP), CAP), pl.ds(pl.multiple_of(cc * 128, 128), 128)]
        dst = home.at[pl.ds(pl.multiple_of(ep * CAP, CAP), CAP), :]
        there = c * 16 + j
        here = (there == ep) & (cc == c)

        @pl.when(here)
        def _():
            pltpu.make_async_copy(src, dst, rt_r).start()

        @pl.when(jnp.logical_not(here))
        def _():
            rdma(src, dst, rt_s, rt_r, (there, 2 * y + cc)).start()

        return 0

    for h in range(HALF):
        res[h * ROWS : (h + 1) * ROWS] = rs_last(h, exp_part, erb, es_r).astype(bf16)
        lax.fori_loop(h * (32 // HALF), (h + 1) * (32 // HALF), send_home, 0)

    rs_step(2, mix_part, msb, mrb, ms_s, ms_r)
    rs_step(3, mix_part, msb, mrb, ms_s, ms_r)
    for h in range(HALF):
        tmo[:, h * (2048 // HALF) : (h + 1) * (2048 // HALF)] = rs_last(h, mix_part, mrb, ms_r).astype(bf16)
    got(home, rt_r)
    eo[...] = (dotb(wch[...], home[...]) + dotb(wcl[...], home[...])).astype(bf16)

    for copy in swaps:
        copy.wait_send()
    for copy in x_copies:
        copy.wait_send()
    for rr in range(1, NZ):

        @pl.when(z + rr < NZ)
        def _():
            sent(ztot, zg_s.at[rr])

    pair.wait_send()

    @pl.when(half == c)
    def _():
        sent(dbuf.at[0:496], dsp_s)
        sent(home.at[0:496], rt_s)

    @pl.when(half != c)
    def _():
        sent(dbuf, dsp_s)
        sent(home, rt_s)

    for d in range(2):
        for h in range(HALF):
            for s in range(length(d, h)):
                if s == 0 or (s == 1 and h % 2 == d):
                    ag_copy(d, h, s).wait_send()
                sent(msb.at[d, h, s], ms_s.at[d, h, s])
                sent(esb.at[d, h, s], es_s.at[d, h, s])


def local(
    receptance, key_matrix, value_matrix, decay_data_term, correction_rate_data, output_gate_input,
    decay_channel_offset, correction_rate_offset, extra_head_log_decay, head_norm_gain, mixer_output_weight,
    expert_layer_input, feedforward_norm_gain, group_router_weight, expert_router_weight, routes,
    expert_gate_weight, expert_up_weight, expert_down_weight,
):
    V = pltpu.VMEM
    DMA = pltpu.SemaphoreType.DMA
    ring = (2, HALF, 4)
    vm = pl.BlockSpec(memory_space=pltpu.VMEM)
    anyw = pl.BlockSpec(memory_space=pl.ANY)
    return pl.pallas_call(
        whole,
        out_shape=(
            jax.ShapeDtypeStruct((32, 2048), bf16),
            jax.ShapeDtypeStruct((128, 128), bf16),
        ),
        in_specs=[vm] * 16 + [anyw] * 4,
        out_specs=(vm, vm),
        scratch_shapes=[
            V((2, 4, 2, 2, 128, 256), bf16), V((2, 4, 2, 2, 128, 256), bf16), V((2, 256, 2048), bf16), V((HD, 2048), bf16),
            DMA((5,)), DMA((6,)), DMA((6,)),
            V((512, 256), bf16), V((256, 2048), bf16), V((128, 512), bf16), V((128, 512), bf16), DMA, DMA, DMA(ring), DMA(ring),
            V((4, 2 * HD, CH), f32), V((4, 2 * HD, HD), f32), V((NX, HD, 2 * HD), bf16), DMA((NX,)), DMA((NX,)),
            V((NZ, HD, 2 * HD), bf16), V((HD, 2 * HD), bf16), DMA((NZ,)), DMA((NZ,)),
            V((NY, 2, 32, HD), bf16), V((NY, 32, HD), bf16), DMA, DMA, V((NY, 32, 2048), f32),
            V((*ring, 32, 2048 // HALF), bf16), V((*ring, 32, 2048 // HALF), bf16), DMA(ring), DMA(ring),
            V((256, 512), bf16), V((NY, 256, 256), f32), V((*ring, ROWS, 256), bf16), V((*ring, ROWS, 256), bf16), DMA(ring), DMA(ring),
            V((256, 256), bf16), V((512, 128), bf16), DMA, DMA,
        ],
        compiler_params=pltpu.CompilerParams(has_side_effects=True, collective_id=0, vmem_limit_bytes=60000 * 1024),
    )(
        receptance.T, key_matrix.T, value_matrix.T, decay_data_term.T, correction_rate_data.T, output_gate_input.T,
        decay_channel_offset.reshape(1, HD), correction_rate_offset.reshape(1, HD), extra_head_log_decay.T,
        head_norm_gain.reshape(1, HD), mixer_output_weight, expert_layer_input, feedforward_norm_gain.reshape(1, 2048),
        group_router_weight.T, expert_router_weight.T, routes.T,
        expert_gate_weight.reshape(2, 4, 2, 128, 256), expert_up_weight.reshape(2, 4, 2, 128, 256), expert_down_weight[0], mixer_output_weight,
    )


def solution(mesh):
    in_specs = (
        P("ep", "tp"), P("ep", "tp"), P("ep", "tp"), P("ep", "tp"), P("ep", "tp"), P("ep", "tp"),
        P("tp"), P("tp"), P("ep", "tp"), P("tp"), P("tp", None),
        P("ep", None), P(), P(), P(), P("ep", None),
        P("ep", None, "tp"), P("ep", None, "tp"), P("ep", "tp", None),
    )
    out_specs = (P(("ep", "tp"), None), P("ep", "tp"))
    return jax.shard_map(local, mesh=mesh, in_specs=in_specs, out_specs=out_specs, check_vma=False)
```

```python
import jax
import jax.numpy as jnp
from jax import lax
from jax.experimental import pallas as pl
from jax.experimental.pallas import tpu as pltpu
from jax.sharding import PartitionSpec as P

f32 = jnp.float32
bf16 = jnp.bfloat16
MESH = pl.DeviceIdType.MESH
HD = 64
CH = 128
NX, NZ, NY = 4, 8, 8
CAP = 16
GROUPS = 4
key_eps = 1e-06
group_eps = 0.00064
norm_eps = 1e-06
HALF = 4
ROWS = 256 // HALF

NN = (((1,), (0,)), ((), ()))
NT = (((1,), (1,)), ((), ()))
TN = (((0,), (0,)), ((), ()))


def dotb(a, b, dims=NN):
    return lax.dot_general(a.astype(bf16), b.astype(bf16), dims, preferred_element_type=f32)


def split(a):
    high = a.astype(bf16)
    return high, (a - high.astype(f32)).astype(bf16)


def dot3(a, b, dims=NN):
    ah, al = split(a)
    bh, bl = split(b)
    return dotb(ah, bh, dims) + (dotb(ah, bl, dims) + dotb(al, bh, dims))


def dot_left2(a, b, dims=NN):
    ah, al = split(a)
    return dotb(ah, b, dims) + dotb(al, b, dims)


def sigmoid(x):
    return 1.0 / (1.0 + jnp.exp(-x))


def iota(shape, dim):
    return lax.broadcasted_iota(jnp.int32, shape, dim)


def column(row):
    n = row.shape[1]
    return jnp.sum(jnp.where(iota((n, n), 0) == iota((n, n), 1), row, 0.0), axis=1, keepdims=True)


def chunk_pairs(r, k, v, dd, cr, doff, coff, extra):
    C = r.shape[1]
    row, col = iota((C, C), 0), iota((C, C), 1)
    u = k * lax.rsqrt(jnp.sum(k * k, axis=0, keepdims=True) + key_eps)
    a = u * sigmoid(cr + coff)
    lg = extra - 0.6065306597126334 * sigmoid(dd + doff)
    lh, lr = split(lg)
    lm, ll = split(lg - lh.astype(f32))
    tri = jnp.where(row <= col, 1.0, 0.0).astype(bf16)
    cum = dotb(lh, tri) + (dotb(lm, tri) + dotb(ll, tri))
    bef = cum - lg
    tot = cum[:, C - 1 : C]
    ref = 0.5 * tot
    en = jnp.exp(ref - cum)
    lhs = jnp.concatenate([u * jnp.exp(bef - ref), r * jnp.exp(cum - ref)], axis=1)
    rhs = jnp.concatenate([k * en, a * en], axis=1)
    G = dotb(lhs, rhs, TN)
    strict, upto = row > col, row >= col
    kp = jnp.where(strict, G[:C, :C], 0.0)
    A = jnp.where(strict, G[:C, C:], 0.0)
    rk = jnp.where(upto, G[C:, :C], 0.0)
    rr = jnp.where(upto, G[C:, C:], 0.0)
    R = jnp.concatenate([dotb(v, kp, NT), u * jnp.exp(bef)], axis=0)
    out = jnp.concatenate([dotb(v, rk, NT), r * jnp.exp(cum)], axis=0)
    tail = jnp.exp(tot - cum)
    diag = jnp.where(iota((HD, HD), 0) == iota((HD, HD), 1), jnp.exp(tot), 0.0)
    bm = jnp.concatenate([dotb(v, k * tail, NT), diag], axis=0)
    return A, R, out, rr, bm, a * tail


def inverses(pairs):
    C = pairs[0].shape[0]
    x = iota((C, C), 0) ^ iota((C, C), 1)
    found = [jnp.where(x == 0, 1.0, 0.0) - jnp.where(x == 1, A, 0.0) for A in pairs]
    s = 2
    while s < C:
        level = (x >= s) & (x < 2 * s)
        right = [dot3(jnp.where(level, A, 0.0), T) for A, T in zip(pairs, found)]
        found = [T - dot3(T, m) for T, m in zip(found, right)]
        s *= 2
    return found


def chunk_ends(T, R, out, rr, bm, at):
    X = dotb(R, T, NT)
    return out - dotb(X, rr, NT), bm - dotb(X, at, NT)


def whole(
    rT, kT, vT, ddT, crT, gateT, doff, coff, extraT, gain, wmix, xin, fgain, grw, erw, routes,
    wg_hbm, wu_hbm, wd_hbm, wmix_hbm,
    tmo, eo,
    wg, wu, wd, wmp, wload, wsend, wrecv,
    dbuf, X, wch, wcl, dsp_s, dsp_r, ag_s, ag_r,
    outT, qp, xg, xg_s, xg_r, zg, ztot, zg_s, zg_r,
    mx, mxp, mx_s, mx_r, pm, msb, mrb, ms_s, ms_r,
    hid, epm, esb, erb, es_s, es_r, res, home, rt_s, rt_r,
):
    ep, tp = lax.axis_index("ep"), lax.axis_index("tp")
    y, c = tp // 2, tp % 2
    z, x = ep // NX, ep % NX
    half, seat = ep // 16, ep % 16
    partner = (ep, tp + 1 - 2 * c)

    def rdma(src, dst, ssem, rsem, device):
        return pltpu.make_async_remote_copy(
            src_ref=src, dst_ref=dst, send_sem=ssem, recv_sem=rsem, device_id=device, device_id_type=MESH
        )

    def got(ref, sem):
        rdma(ref, ref, sem, sem, partner).wait_recv()

    def sent(ref, sem):
        rdma(ref, ref, sem, sem, partner).wait_send()

    barrier = pltpu.get_barrier_semaphore()

    def greet(device):
        pl.semaphore_signal(barrier, inc=1, device_id=device, device_id_type=MESH)

    def meet(e, _):
        @pl.when(jnp.logical_not((e == ep) & (half == c)))
        def _():
            greet((e, 2 * y + half))

        there, cc = c * 16 + e // 2, e % 2

        @pl.when(jnp.logical_not((there == ep) & (cc == c)))
        def _():
            greet((there, 2 * y + cc))

        return 0

    lax.fori_loop(0, 32, meet, 0)
    greet(partner)
    for d in (1, NY - 1):
        greet((ep, 2 * ((y + d) % NY) + c))
    for d in range(1, NX):
        greet((z * NX + (x + d) % NX, tp))
    for d in range(1, NZ):
        greet(((z + d) % NZ * NX + x, tp))

    loads, swaps = [], []
    for n, (hbm, dst) in enumerate(((wg_hbm, wg), (wu_hbm, wu))):
        for q in range(2):
            loads.append(pltpu.make_async_copy(hbm.at[q], dst.at[0, :, :, q], wload.at[2 * n + q]))
            swaps.append(rdma(hbm.at[q], dst.at[1, :, :, q], wsend.at[2 * n + q], wrecv.at[2 * n + q], partner))
    loads.append(pltpu.make_async_copy(wd_hbm, wd.at[0], wload.at[4]))
    swaps.append(rdma(wd_hbm, wd.at[1], wsend.at[4], wrecv.at[4], partner))
    swaps.append(rdma(wmix_hbm, wmp, wsend.at[5], wrecv.at[5], partner))
    for copy in loads:
        copy.start()

    xf = xin[...].astype(f32)
    rs = lax.rsqrt(jnp.mean(xf * xf, axis=-1, keepdims=True) + norm_eps)
    r0, r1 = routes[0:1, :], routes[1:2, :]
    experts = iota((32, 128), 0)
    m0 = jnp.where(r0 == experts, 1.0, 0.0)
    m1 = jnp.where(r1 == experts, 1.0, 0.0)
    before = jnp.where(iota((128, 128), 0) < iota((128, 128), 1), 1.0, 0.0)
    rank = dotb(m0 + m1, before)
    spread = jnp.where(iota((512, 32), 0) // CAP == iota((512, 32), 1), 1.0, 0.0)
    placed = jnp.where(dotb(spread, rank) == (iota((512, 128), 0) % CAP).astype(f32), dotb(spread, m0 + m1), 0.0)
    fours = y % 4
    for q in range(2):
        cols = pl.ds(pl.multiple_of((2 * fours + 8 * q + c) * 128, 128), 128)
        mine = (xin[:, cols].astype(f32) * rs * fgain[:, cols]).astype(bf16)
        dbuf[:, q * 128 : (q + 1) * 128] = dotb(placed, mine).astype(bf16)

    def dispatch(e, _):
        src = dbuf.at[pl.ds(pl.multiple_of(e * CAP, CAP), CAP), :]
        dst = X.at[
            pl.ds(pl.multiple_of(seat * CAP, CAP), CAP), pl.ds(pl.multiple_of(fours * 512 + c * 256, 128), 256)
        ]
        here = (e == ep) & (half == c)

        @pl.when(here)
        def _():
            pltpu.make_async_copy(src, dst, dsp_r).start()

        @pl.when(jnp.logical_not(here))
        def _():
            rdma(src, dst, dsp_s, dsp_r, (e, 2 * y + half)).start()

        return 0

    def length(d, h):
        return 4 if d == h % 2 else 3

    def at_y(v):
        return (v + 2 * NY) % NY

    def neighbour(d):
        return (ep, 2 * at_y(y + 1 - 2 * d) + c)

    def lanes(s):
        return pl.ds(pl.multiple_of(s * 256, 256), 256)

    def ag_block(place, h):
        return X.at[h * ROWS : (h + 1) * ROWS, pl.ds(pl.multiple_of(at_y(place) % 4 * 512, 512), 512)]

    def behind(d):
        return y - 1 if d == 0 else y + 1

    def ag_copy(d, h, s):
        ref = ag_block(y if s == 0 else behind(d), h)
        return rdma(ref, ref, ag_s.at[d, h, s], ag_r.at[d, h, s], neighbour(d))

    def ag_first():
        for h in range(HALF):
            for d in (h % 2, 1 - h % 2):
                ag_copy(d, h, 0).start()

    def ag_second():
        for h in range(HALF):
            for d in (h % 2, 1 - h % 2):
                got(ag_block(behind(d), h), ag_r.at[d, h, 0])
                if h % 2 == d:
                    ag_copy(d, h, 1).start()

    def ag_done():
        for h in range(HALF):
            got(ag_block(y + 2, h), ag_r.at[h % 2, h, 1])

    def local_chunks(numbers):
        pairs = []
        for n in numbers:
            sl = slice(n * CH, (n + 1) * CH)
            pairs.append(
                chunk_pairs(
                    rT[:, sl].astype(f32), kT[:, sl].astype(f32), vT[:, sl].astype(f32), ddT[:, sl].astype(f32),
                    crT[:, sl].astype(f32), column(doff[...]), column(coff[...]), extraT[:, sl],
                )
            )
        bms = []
        for n, T, p in zip(numbers, inverses([p[0] for p in pairs]), pairs):
            outT[n], bm = chunk_ends(T, *p[1:])
            bms.append(bm)
        return bms

    upper = iota((2 * HD, HD), 0)
    across = iota((2 * HD, HD), 1)

    def join(stack, later_q, later_p):
        return dot_left2(stack, later_p) + jnp.concatenate([later_q, jnp.zeros((HD, HD), f32)], axis=0)

    def rs_step(s, part, sbuf, rbuf, ssem, rsem):
        for h in range(HALF):
            for d in range(2):
                n = length(d, h)
                if s >= n:
                    continue
                dest = at_y(y + (n - s) if d == 0 else y - (n - s))
                value = part(dest, h)
                if s > 0:
                    got(rbuf.at[d, h, s - 1], rsem.at[d, h, s - 1])
                    value = value + rbuf[d, h, s - 1].astype(f32)
                sbuf[d, h, s] = value.astype(bf16)
                rdma(sbuf.at[d, h, s], rbuf.at[d, h, s], ssem.at[d, h, s], rsem.at[d, h, s], neighbour(d)).start()

    def rs_last(h, part, rbuf, rsem):
        value = part(y, h)
        for d in range(2):
            n = length(d, h) - 1
            got(rbuf.at[d, h, n], rsem.at[d, h, n])
            value = value + rbuf[d, h, n].astype(f32)
        return value

    def mix_part(dest, h):
        return pm[dest, :, h * (2048 // HALF) : (h + 1) * (2048 // HALF)]

    @pl.when(half == c)
    def _():
        pl.semaphore_wait(barrier, 62 + 3 + NX - 1 + NZ - 1)

    @pl.when(half != c)
    def _():
        pl.semaphore_wait(barrier, 64 + 3 + NX - 1 + NZ - 1)

    lax.fori_loop(0, 32, dispatch, 0)
    for copy in swaps:
        copy.start()

    bms = local_chunks((0, 1, 2, 3))
    stack = jnp.where(upper == across + HD, 1.0, 0.0)
    for n in range(4):
        qp[n] = stack
        stack = dot3(stack, bms[n][HD:]) + jnp.where(upper < HD, bms[n], 0.0)
    xg[0] = jnp.concatenate([stack[:HD], stack[HD:]], axis=1).astype(bf16)
    x_copies = []
    for rr in range(1, NX):
        to = (z * NX + (x + rr) % NX, tp)
        x_copies.append(rdma(xg.at[0], xg.at[rr], xg_s.at[rr], xg_r.at[rr], to))
        x_copies[-1].start()

    got(X.at[:, pl.ds(pl.multiple_of(fours * 512, 512), 512)], dsp_r)
    ag_first()
    for rr in range(1, NX):
        got(xg.at[rr], xg_r.at[rr])
    stack = jnp.where(upper == across + HD, 1.0, 0.0)
    own_q, own_p = jnp.zeros((HD, HD), f32), jnp.zeros((HD, HD), f32)
    for i in range(NX):
        own_q = jnp.where(x == i, stack[:HD], own_q)
        own_p = jnp.where(x == i, stack[HD:], own_p)
        piece = xg[(x - i + NX) % NX].astype(f32)
        stack = join(stack, piece[:, :HD], piece[:, HD:])
    ztot[...] = jnp.concatenate([stack[:HD], stack[HD:]], axis=1).astype(bf16)
    for rr in range(1, NZ):

        @pl.when(z + rr < NZ)
        def _():
            rdma(ztot, zg.at[z], zg_s.at[rr], zg_r.at[z], ((z + rr) * NX + x, tp)).start()

    ag_second()
    nb = (xf * rs * fgain[...]).astype(bf16)
    logit = dotb(erw[...], nb, NT)
    gexp = jnp.exp(dotb(grw[...], nb, NT))
    gprob = gexp / jnp.sum(gexp, axis=0, keepdims=True)
    c0 = jnp.sum(jnp.where(r0 == experts, logit, 0.0), axis=0, keepdims=True)
    c1 = jnp.sum(jnp.where(r1 == experts, logit, 0.0), axis=0, keepdims=True)
    groups = iota((GROUPS, 128), 0)
    g0 = jnp.sum(jnp.where(r0 // 8 == groups, gprob, 0.0), axis=0, keepdims=True)
    g1 = jnp.sum(jnp.where(r1 // 8 == groups, gprob, 0.0), axis=0, keepdims=True)
    weight = m0 * (g0 * sigmoid(c0 - c1)) + m1 * (g1 * sigmoid(c1 - c0))
    wh, wl = split(weight)
    full = placed * (dotb(spread, wh) + dotb(spread, wl))
    fh, fl = split(full.T)
    wch[...] = fh
    wcl[...] = fl

    ag_done()
    for copy in loads:
        copy.wait()
    for copy in swaps[:5]:
        copy.wait_recv()
    for q in range(2):
        g = dotb(X[...], wg[q].reshape(2048, 256))
        u = dotb(X[...], wu[q].reshape(2048, 256))
        hid[:, q * 256 : (q + 1) * 256] = (g * sigmoid(g) * u).astype(bf16)

    def down(shift):
        dest = at_y(y + shift)
        epm[dest] = dotb(hid[:, :256], wd[0, :, lanes(dest)]) + dotb(hid[:, 256:], wd[1, :, lanes(dest)])

    def exp_part(dest, h):
        return epm[dest, h * ROWS : (h + 1) * ROWS]

    for shift in (4, 3, -3):
        down(shift)
    rs_step(0, exp_part, esb, erb, es_s, es_r)
    def fold(i, state):
        got(zg.at[i], zg_r.at[i])
        piece = zg[i].astype(f32)
        return dot_left2(state, piece[:, HD:]) + piece[:, :HD]

    state = lax.fori_loop(0, z, fold, jnp.zeros((HD, HD), f32))
    state = dot3(state, own_p) + own_q
    gain_c = column(gain[...])
    for n in range(4):
        sl = slice(n * CH, (n + 1) * CH)
        q = qp[n]
        now = dot3(state, q[HD:]) + q[:HD]
        o = outT[n]
        ho = o[:HD] + dotb(now, o[HD:])
        ho = ho - jnp.mean(ho, axis=0, keepdims=True)
        sp = jnp.mean(ho * ho, axis=0, keepdims=True)
        mixed = ho * lax.rsqrt(sp + group_eps) * gain_c * sigmoid(gateT[:, sl].astype(f32))
        mx[2 * n : 2 * n + 2] = mixed.T.reshape(2, 2, 32, HD).astype(bf16)
    pair = rdma(mx.at[:, 1 - c], mxp, mx_s, mx_r, partner)
    pair.start()
    for shift in (2, -2):
        down(shift)
    rs_step(1, exp_part, esb, erb, es_s, es_r)
    pair.wait_recv()
    swaps[5].wait_recv()
    total = dotb(mx[:, c].reshape(256, HD), wmix[...]) + dotb(mxp[...].reshape(256, HD), wmp[...])
    pm[...] = total.reshape(NY, 32, 2048)

    rs_step(0, mix_part, msb, mrb, ms_s, ms_r)
    for shift in (1, -1, 0):
        down(shift)
    rs_step(2, exp_part, esb, erb, es_s, es_r)
    rs_step(1, mix_part, msb, mrb, ms_s, ms_r)
    rs_step(3, exp_part, esb, erb, es_s, es_r)
    def send_home(n, _):
        j, cc = n // 2, n % 2
        src = res.at[pl.ds(pl.multiple_of(j * CAP, CAP), CAP), pl.ds(pl.multiple_of(cc * 128, 128), 128)]
        dst = home.at[pl.ds(pl.multiple_of(ep * CAP, CAP), CAP), :]
        there = c * 16 + j
        here = (there == ep) & (cc == c)

        @pl.when(here)
        def _():
            pltpu.make_async_copy(src, dst, rt_r).start()

        @pl.when(jnp.logical_not(here))
        def _():
            rdma(src, dst, rt_s, rt_r, (there, 2 * y + cc)).start()

        return 0

    for h in range(HALF):
        res[h * ROWS : (h + 1) * ROWS] = rs_last(h, exp_part, erb, es_r).astype(bf16)
        lax.fori_loop(h * (32 // HALF), (h + 1) * (32 // HALF), send_home, 0)

    rs_step(2, mix_part, msb, mrb, ms_s, ms_r)
    rs_step(3, mix_part, msb, mrb, ms_s, ms_r)
    got(home, rt_r)
    eo[...] = (dotb(wch[...], home[...]) + dotb(wcl[...], home[...])).astype(bf16)

    for h in range(HALF):
        tmo[:, h * (2048 // HALF) : (h + 1) * (2048 // HALF)] = rs_last(h, mix_part, mrb, ms_r).astype(bf16)
    for copy in swaps:
        copy.wait_send()
    for copy in x_copies:
        copy.wait_send()
    for rr in range(1, NZ):

        @pl.when(z + rr < NZ)
        def _():
            sent(ztot, zg_s.at[rr])

    pair.wait_send()

    @pl.when(half == c)
    def _():
        sent(dbuf.at[0:496], dsp_s)
        sent(home.at[0:496], rt_s)

    @pl.when(half != c)
    def _():
        sent(dbuf, dsp_s)
        sent(home, rt_s)

    for d in range(2):
        for h in range(HALF):
            for s in range(length(d, h)):
                if s == 0 or (s == 1 and h % 2 == d):
                    ag_copy(d, h, s).wait_send()
                sent(msb.at[d, h, s], ms_s.at[d, h, s])
                sent(esb.at[d, h, s], es_s.at[d, h, s])


def local(
    receptance, key_matrix, value_matrix, decay_data_term, correction_rate_data, output_gate_input,
    decay_channel_offset, correction_rate_offset, extra_head_log_decay, head_norm_gain, mixer_output_weight,
    expert_layer_input, feedforward_norm_gain, group_router_weight, expert_router_weight, routes,
    expert_gate_weight, expert_up_weight, expert_down_weight,
):
    V = pltpu.VMEM
    DMA = pltpu.SemaphoreType.DMA
    ring = (2, HALF, 4)
    vm = pl.BlockSpec(memory_space=pltpu.VMEM)
    anyw = pl.BlockSpec(memory_space=pl.ANY)
    return pl.pallas_call(
        whole,
        out_shape=(
            jax.ShapeDtypeStruct((32, 2048), bf16),
            jax.ShapeDtypeStruct((128, 128), bf16),
        ),
        in_specs=[vm] * 16 + [anyw] * 4,
        out_specs=(vm, vm),
        scratch_shapes=[
            V((2, 4, 2, 2, 128, 256), bf16), V((2, 4, 2, 2, 128, 256), bf16), V((2, 256, 2048), bf16), V((HD, 2048), bf16),
            DMA((5,)), DMA((6,)), DMA((6,)),
            V((512, 256), bf16), V((256, 2048), bf16), V((128, 512), bf16), V((128, 512), bf16), DMA, DMA, DMA(ring), DMA(ring),
            V((4, 2 * HD, CH), f32), V((4, 2 * HD, HD), f32), V((NX, HD, 2 * HD), bf16), DMA((NX,)), DMA((NX,)),
            V((NZ, HD, 2 * HD), bf16), V((HD, 2 * HD), bf16), DMA((NZ,)), DMA((NZ,)),
            V((NY, 2, 32, HD), bf16), V((NY, 32, HD), bf16), DMA, DMA, V((NY, 32, 2048), f32),
            V((*ring, 32, 2048 // HALF), bf16), V((*ring, 32, 2048 // HALF), bf16), DMA(ring), DMA(ring),
            V((256, 512), bf16), V((NY, 256, 256), f32), V((*ring, ROWS, 256), bf16), V((*ring, ROWS, 256), bf16), DMA(ring), DMA(ring),
            V((256, 256), bf16), V((512, 128), bf16), DMA, DMA,
        ],
        compiler_params=pltpu.CompilerParams(has_side_effects=True, collective_id=0, vmem_limit_bytes=60000 * 1024),
    )(
        receptance.T, key_matrix.T, value_matrix.T, decay_data_term.T, correction_rate_data.T, output_gate_input.T,
        decay_channel_offset.reshape(1, HD), correction_rate_offset.reshape(1, HD), extra_head_log_decay.T,
        head_norm_gain.reshape(1, HD), mixer_output_weight, expert_layer_input, feedforward_norm_gain.reshape(1, 2048),
        group_router_weight.T, expert_router_weight.T, routes.T,
        expert_gate_weight.reshape(2, 4, 2, 128, 256), expert_up_weight.reshape(2, 4, 2, 128, 256), expert_down_weight[0], mixer_output_weight,
    )


def solution(mesh):
    in_specs = (
        P("ep", "tp"), P("ep", "tp"), P("ep", "tp"), P("ep", "tp"), P("ep", "tp"), P("ep", "tp"),
        P("tp"), P("tp"), P("ep", "tp"), P("tp"), P("tp", None),
        P("ep", None), P(), P(), P(), P("ep", None),
        P("ep", None, "tp"), P("ep", None, "tp"), P("ep", "tp", None),
    )
    out_specs = (P(("ep", "tp"), None), P("ep", "tp"))
    return jax.shard_map(local, mesh=mesh, in_specs=in_specs, out_specs=out_specs, check_vma=False)
```
